32 devices in a mesh: sp: 8 (over z, y), tp: 4 (over x, core).
Axes of the slice: x: 2, y: 2, z: 4, core: 2. Of those that a mesh axis runs over, the one named last changes fastest.
Arguments:
- query_rows: bfloat16 [4096, 2048], P('sp', 'tp'), may hold values from -40 to 40
- key_rows: bfloat16 [4096, 256], P('sp', 'tp'), may hold values from -6 to 6
- value_rows: bfloat16 [4096, 256], P('sp', 'tp'), may hold values from -12 to 12
- doc_ids: int32 [4096], P('sp'), may hold values from 0 to 3, never falling along the last dimension, each value on 1 to 2048 neighbouring positions
- sink_logit: float32 [32], P('tp'), may hold values from 1 to 6
- residual: bfloat16 [4096, 2048], P('sp'), may hold values from -10 to 10
- out_proj: bfloat16 [2048, 2048], P('tp'), may hold values from -0.25 to 0.25
- mix_gain: float32 [2048], replicated, may hold values from 0.1 to 1.9
- gate_proj: bfloat16 [2048, 5632], P('sp', 'tp'), may hold values from -0.125 to 0.125
- value_proj: bfloat16 [2048, 5632], P('sp', 'tp'), may hold values from -0.125 to 0.125
- gate_taps: float32 [3, 5632], P(None, 'tp'), may hold values from -3 to 3
- value_taps: float32 [3, 5632], P(None, 'tp'), may hold values from -3 to 3
- down_proj: bfloat16 [5632, 2048], P('tp', 'sp'), may hold values from -0.078125 to 0.078125
- final_gain: float32 [2048], P('tp'), may hold values from 0.1 to 1.9
Outputs:
- mixed: bfloat16 [4096, 2048], P('sp', 'tp')
The draws below stay inside these ranges and needn't reach their ends.
All inputs are finite; a program needn't handle non-finite values.
Results may differ from the reference program's by a relative error of at most 0.012.
Values may be sent and summed in bfloat16 or wider, within the bound.
A program may use at most 128 MiB of HBM per device.

```python
import math
import jax
import jax.numpy as jnp
import numpy as np
from jax import lax

D = 2048
HQ = 32
HK = 4
HD = 64
FF = 5632
WIN = 128
TAPS = 3
TOK_DEV = 512
TOKENS = 4096
DOC_COUNT = 4
DOC_MOST = 2048
N_TP = 4


def draw_key_rows(key, part):
    drawn = jax.random.truncated_normal(jax.random.fold_in(key, 1), -6.0, 6.0, (TOKENS, HK, HD), jnp.float32)
    return drawn.reshape(TOKENS, HK * HD).astype(jnp.bfloat16)


def draw_query_rows(key, part):
    drawn = jax.random.truncated_normal(jax.random.fold_in(key, 3), -6.0, 6.0, (TOKENS, HQ, HD), jnp.float32)
    return drawn.reshape(TOKENS, HQ * HD).astype(jnp.bfloat16)


def draw_residual(key, part):
    columns = jnp.arange(D, dtype=jnp.float32) / max(D - 1, 1)
    base = 0.4 * jax.random.truncated_normal(key, -6.0, 6.0, (TOKENS, D), jnp.float32)
    scale = jnp.exp(columns * math.log(4.0))
    return (base * scale[None, :]).astype(jnp.bfloat16)


def levels(stream_key, shape, pieces, smallest, largest):
    level, own = 1.0, jax.random.fold_in(stream_key, 6)
    for position, shards_of in pieces:
        steps = jnp.exp(jax.random.uniform(jax.random.fold_in(own, position), (shards_of,), jnp.float32, smallest / len(pieces), largest / len(pieces)))
        level = level * jnp.repeat(steps, shape[position] // shards_of).reshape([-1 if axis == position else 1 for axis in range(len(shape))])
    return level


def split_up(number_of, total, reach, skew):
    loads = [(1 << 20) // math.isqrt(standing ** skew) + 1 for standing in range(2, number_of + 1)]
    rest, holding = total - reach - (number_of - 1), [1] * (number_of - 1)
    while rest > 0:
        candidates = [i for i in range(number_of - 1) if holding[i] < reach]
        whole, left = sum([loads[i] for i in candidates]), rest
        for i in candidates:
            extra = min(reach - holding[i], max(1, left * loads[i] // whole), rest)
            holding[i] = holding[i] + extra
            rest = rest - extra
    return np.array([reach] + holding)


def uneven_parts(stream_key, count, total, most, slope):
    if count == 2:
        one = jax.random.randint(stream_key, (), max(1, total - most), min(most, total - 1) + 1)
        return jnp.stack([one, total - one])
    tallies = jnp.asarray(split_up(count, total, most, slope), jnp.int32)
    couples = (count - 1) // 2
    source_of, receiver = tallies[1:1 + 2 * couples:2], tallies[2:2 + 2 * couples:2]
    slack = jnp.minimum(source_of - 1, most - receiver)
    moved = jax.random.randint(jax.random.fold_in(stream_key, 1), (couples,), 0, 1 << 20) % (slack + 1)
    tallies = tallies.at[1:1 + 2 * couples:2].set(source_of - moved).at[2:2 + 2 * couples:2].set(receiver + moved)
    return tallies[jax.random.permutation(jax.random.fold_in(stream_key, 2), count)]


def noise(key, dims, scale, limit, pieces=(), kind=jnp.bfloat16):
    result = scale * jax.random.normal(key, dims, jnp.float32)
    if pieces:
        result = result * levels(key, dims, pieces, -0.22, 0.18)
    return jnp.clip(result, -limit, limit).astype(kind)


def setup_inputs(seed: int = 0) -> dict:
    arg_keys = jax.random.split(jax.random.key(seed), 15)
    return {
        "query_rows": draw_query_rows(jax.random.fold_in(arg_keys[14], 71), 0),
        "key_rows": draw_key_rows(jax.random.fold_in(arg_keys[14], 71), 0),
        "value_rows": noise(arg_keys[2], (TOKENS, HK * HD), 2.0, 12.0, ((0, 8), (1, 4))),
        "doc_ids": jnp.searchsorted(jnp.cumsum(uneven_parts(arg_keys[3], DOC_COUNT, TOKENS, DOC_MOST, 2)), jnp.arange(TOKENS), side="right").astype(jnp.int32),
        "sink_logit": jnp.clip(1.0 + 5.0 * jax.random.uniform(arg_keys[4], (HQ,), jnp.float32) ** levels(arg_keys[4], (HQ,), ((0, 4),), -0.2, 0.2), 1.0, 6.0),
        "residual": draw_residual(jax.random.fold_in(arg_keys[14], 71), 0),
        "out_proj": noise(arg_keys[6], (HQ * HD, D), (HQ * HD // 4) ** -0.5, 0.25, ((0, 4),)),
        "mix_gain": jnp.clip(1.0 + 0.18 * jax.random.normal(arg_keys[7], (D,), jnp.float32), 0.1, 1.9),
        "gate_proj": noise(arg_keys[8], (D, FF), D ** -0.5, 0.125, ((0, 8), (1, 4))),
        "value_proj": noise(arg_keys[9], (D, FF), D ** -0.5, 0.125, ((0, 8), (1, 4))),
        "gate_taps": noise(arg_keys[10], (TAPS, FF), 0.6, 3.0, ((1, 4),), jnp.float32),
        "value_taps": noise(arg_keys[11], (TAPS, FF), 0.6, 3.0, ((1, 4),), jnp.float32),
        "down_proj": noise(arg_keys[12], (FF, D), FF ** -0.5, 0.078125, ((0, 4), (1, 8))),
        "final_gain": jnp.clip(1.0 + 0.18 * jax.random.normal(arg_keys[13], (D,), jnp.float32), 0.1, 1.9),
    }


mix_scale = math.sqrt(2.0)
norm_eps = 1e-05

def attend(query_block, key_block, value_block, query_pos, key_pos, query_doc, key_doc, sink):
    head_size = query_block.shape[-1]
    scores = jnp.einsum('qkgd,skd->kgqs', query_block.astype(jnp.float32), key_block.astype(jnp.float32)) * head_size ** (-0.5)
    diff = query_pos[:, None] - key_pos[None, :]
    valid = (diff >= 0) & (diff < WIN) & (query_doc[:, None] == key_doc[None, :]) & (key_pos[None, :] >= 0)
    scores = jnp.where(valid[None, None], scores, -1e+30)
    top = jnp.maximum(lax.optimization_barrier(jnp.max(scores, axis=-1, keepdims=True)), sink)
    weights = jnp.exp(scores - top)
    total = lax.optimization_barrier(jnp.sum(weights, axis=-1, keepdims=True)) + jnp.exp(sink - top)
    probs = (weights / total).astype(jnp.bfloat16)
    out = jnp.einsum('kgqs,skd->qkgd', probs.astype(jnp.float32), value_block.astype(jnp.float32))
    return out.astype(jnp.bfloat16)

def depthwise(tail, current, taps, tail_docs, docs):
    extended = jnp.concatenate([tail, current])
    ext_docs = jnp.concatenate([tail_docs, docs])
    lag_rows = tail.shape[0]
    count = current.shape[0]
    total = jnp.zeros(current.shape, jnp.float32)
    for lag in range(lag_rows + 1):
        start = lag_rows - lag
        same = (ext_docs[start:start + count] == docs)[:, None]
        rows = extended[start:start + count].astype(jnp.float32)
        total = total + taps[lag].astype(jnp.float32)[None, :] * jnp.where(same, rows, 0.0)
    return total

def layer_norm(values, gain):
    mean = lax.optimization_barrier(jnp.mean(values, axis=1, keepdims=True))
    var = lax.optimization_barrier(jnp.mean(jnp.square(values - mean), axis=1, keepdims=True))
    return (values - mean) * lax.rsqrt(var + norm_eps) * gain.astype(jnp.float32)[None, :]

def reference(query_rows, key_rows, value_rows, doc_ids, sink_logit, residual, out_proj, mix_gain, gate_proj, value_proj, gate_taps, value_taps, down_proj, final_gain):
    groups = HQ // HK
    block = min(512, TOK_DEV)
    count = TOKENS // block
    queries = query_rows.reshape(TOKENS, HK, groups, HD)
    pad_keys = jnp.concatenate([jnp.zeros((WIN, HK * HD), jnp.bfloat16), key_rows]).reshape(TOKENS + WIN, HK, HD)
    pad_values = jnp.concatenate([jnp.zeros((WIN, HK * HD), jnp.bfloat16), value_rows]).reshape(TOKENS + WIN, HK, HD)
    docs = doc_ids.astype(jnp.int32)
    pad_docs = jnp.concatenate([jnp.full((WIN,), -1, jnp.int32), docs])
    sink = sink_logit.astype(jnp.float32).reshape(HK, groups, 1, 1)

    def one_block(index):
        start = (index * block).astype(jnp.int32)
        query_block = lax.dynamic_slice_in_dim(queries, start, block, 0)
        key_block = lax.dynamic_slice_in_dim(pad_keys, start, block + WIN, 0)
        value_block = lax.dynamic_slice_in_dim(pad_values, start, block + WIN, 0)
        query_doc = lax.dynamic_slice_in_dim(docs, start, block, 0)
        key_doc = lax.dynamic_slice_in_dim(pad_docs, start, block + WIN, 0)
        query_pos = start + jnp.arange(block, dtype=jnp.int32)
        key_pos = start - WIN + jnp.arange(block + WIN, dtype=jnp.int32)
        return attend(query_block, key_block, value_block, query_pos, key_pos, query_doc, key_doc, sink)
    heads = lax.map(one_block, jnp.arange(count, dtype=jnp.int32)).reshape(TOKENS, HQ * HD)
    head_cols = HQ * HD // N_TP
    attn_proj = jnp.zeros((TOKENS, D), jnp.float32)
    for group in range(N_TP):
        part = jnp.dot(heads[:, group * head_cols:(group + 1) * head_cols], out_proj[group * head_cols:(group + 1) * head_cols], preferred_element_type=jnp.float32)
        attn_proj = attn_proj + part.astype(jnp.bfloat16).astype(jnp.float32)
    first_sum = mix_scale * residual.astype(jnp.float32) + attn_proj
    normed = layer_norm(first_sum, mix_gain).astype(jnp.bfloat16)
    up_gate = jnp.dot(normed, gate_proj, preferred_element_type=jnp.float32).astype(jnp.bfloat16)
    up_value = jnp.dot(normed, value_proj, preferred_element_type=jnp.float32).astype(jnp.bfloat16)
    lag_rows = TAPS - 1
    zero_tail = jnp.zeros((lag_rows, FF), jnp.bfloat16)
    tail_docs = jnp.full((lag_rows,), -1, jnp.int32)
    conv_gate = depthwise(zero_tail, up_gate, gate_taps, tail_docs, docs)
    conv_value = depthwise(zero_tail, up_value, value_taps, tail_docs, docs)
    hidden = (jax.nn.gelu(conv_gate) * conv_value).astype(jnp.bfloat16)
    unit_cols = FF // N_TP
    ffn = jnp.zeros((TOKENS, D), jnp.float32)
    for group in range(N_TP):
        part = jnp.dot(hidden[:, group * unit_cols:(group + 1) * unit_cols], down_proj[group * unit_cols:(group + 1) * unit_cols], preferred_element_type=jnp.float32)
        ffn = ffn + part.astype(jnp.bfloat16).astype(jnp.float32)
    second_sum = mix_scale * normed.astype(jnp.float32) + ffn
    return layer_norm(second_sum, final_gain).astype(jnp.bfloat16)
```

```python
import functools
import math

import jax
import jax.numpy as jnp
from jax import lax
from jax.experimental import pallas as pl
from jax.experimental.pallas import tpu as pltpu
from jax.sharding import PartitionSpec as P

HD = 64
WIN = 128
TAPS = 3


mix_scale = math.sqrt(2.0)
norm_eps = 1e-05


def passed_along(block, axis, distance):
    devices = range(lax.axis_size(axis))
    route = [(i - distance, i) for i in devices if i - distance in devices]
    return lax.ppermute(block, axis, route)


def attend(query_block, key_block, value_block, query_pos, key_pos, query_doc, key_doc, sink):
    head_size = query_block.shape[-1]
    scores = jnp.einsum(
        "qkgd,skd->kgqs", query_block, key_block, preferred_element_type=jnp.float32
    ) * head_size ** (-0.5)
    diff = query_pos[:, None] - key_pos[None, :]
    valid = (
        (diff >= 0)
        & (diff < WIN)
        & (query_doc[:, None] == key_doc[None, :])
        & (key_pos[None, :] >= 0)
    )
    scores = jnp.where(valid[None, None], scores, -1e30)
    top = jnp.maximum(jnp.max(scores, axis=-1, keepdims=True), sink)
    weights = jnp.exp(scores - top)
    total = jnp.sum(weights, axis=-1, keepdims=True) + jnp.exp(sink - top)
    probs = (weights / total).astype(jnp.bfloat16)
    out = jnp.einsum("kgqs,skd->qkgd", probs, value_block, preferred_element_type=jnp.float32)
    return out.astype(jnp.bfloat16)


def depthwise(tail, current, taps, tail_docs, docs):
    extended = jnp.concatenate([tail, current])
    ext_docs = jnp.concatenate([tail_docs, docs])
    lag_rows = tail.shape[0]
    count = current.shape[0]
    total = jnp.zeros(current.shape, jnp.float32)
    for lag in range(lag_rows + 1):
        start = lag_rows - lag
        same = (ext_docs[start : start + count] == docs)[:, None]
        rows = extended[start : start + count].astype(jnp.float32)
        total = total + taps[lag][None, :] * jnp.where(same, rows, 0.0)
    return total


def on_device(
    query_rows,
    key_rows,
    value_rows,
    doc_ids,
    sink_logit,
    residual,
    out_proj,
    mix_gain,
    gate_proj,
    value_proj,
    gate_taps,
    value_taps,
    down_proj,
    final_gain,
):
    rows = query_rows.shape[0]
    kv_local = key_rows.shape[1] // HD
    heads_local = query_rows.shape[1] // HD
    groups = heads_local // kv_local
    offset = lax.axis_index("sp") * rows
    prev_keys, prev_values, prev_docs = passed_along(
        (key_rows[rows - WIN :], value_rows[rows - WIN :], doc_ids[rows - WIN :]), "sp", 1
    )
    all_keys = jnp.concatenate([prev_keys, key_rows]).reshape(rows + WIN, kv_local, HD)
    all_values = jnp.concatenate([prev_values, value_rows]).reshape(rows + WIN, kv_local, HD)
    all_docs = jnp.concatenate([prev_docs, doc_ids])
    key_pos = offset - WIN + jnp.arange(rows + WIN, dtype=jnp.int32)
    query_pos = offset + jnp.arange(rows, dtype=jnp.int32)
    queries = query_rows.reshape(rows, kv_local, groups, HD)
    sink = sink_logit.reshape(kv_local, groups, 1, 1)
    pieces = attend(queries, all_keys, all_values, query_pos, key_pos, doc_ids, all_docs, sink)
    heads = pieces.reshape(rows, heads_local * HD)
    partial_value = jnp.dot(heads, out_proj, preferred_element_type=jnp.float32)
    width = residual.shape[1]
    share = width // lax.axis_size("tp")
    col_start = lax.axis_index("tp") * share
    attn_total = lax.psum(partial_value.astype(jnp.bfloat16), "tp").astype(jnp.float32)
    first_sum = mix_scale * residual.astype(jnp.float32) + attn_total
    mean = jnp.mean(first_sum, axis=1, keepdims=True)
    var = jnp.mean(jnp.square(first_sum - mean), axis=1, keepdims=True)
    normed = ((first_sum - mean) * lax.rsqrt(var + norm_eps) * mix_gain[None, :]).astype(
        jnp.bfloat16
    )
    normed_own = lax.dynamic_slice_in_dim(normed, col_start, share, 1)
    up_gate = jnp.dot(
        normed,
        lax.all_gather(gate_proj, "sp", axis=0, tiled=True),
        preferred_element_type=jnp.float32,
    )
    up_value = jnp.dot(
        normed,
        lax.all_gather(value_proj, "sp", axis=0, tiled=True),
        preferred_element_type=jnp.float32,
    )
    up_gate = up_gate.astype(jnp.bfloat16)
    up_value = up_value.astype(jnp.bfloat16)
    lag_rows = TAPS - 1
    prev_gate, prev_value = passed_along(
        (up_gate[rows - lag_rows :], up_value[rows - lag_rows :]), "sp", 1
    )
    tail_docs = prev_docs[WIN - lag_rows :]
    conv_gate = depthwise(prev_gate, up_gate, gate_taps, tail_docs, doc_ids)
    conv_value = depthwise(prev_value, up_value, value_taps, tail_docs, doc_ids)
    hidden = (jax.nn.gelu(conv_gate) * conv_value).astype(jnp.bfloat16)
    terms = jnp.dot(
        hidden,
        lax.all_gather(down_proj, "sp", axis=1, tiled=True),
        preferred_element_type=jnp.float32,
    )
    ffn_own = lax.psum_scatter(
        terms.astype(jnp.bfloat16), "tp", scatter_dimension=1, tiled=True
    ).astype(jnp.float32)
    second_sum = mix_scale * normed_own.astype(jnp.float32) + ffn_own
    row_sum, row_squares = lax.psum(
        (jnp.sum(second_sum, axis=1), jnp.sum(second_sum * second_sum, axis=1)), "tp"
    )
    mean = row_sum / width
    var = row_squares / width - mean * mean
    return (
        (second_sum - mean[:, None]) * lax.rsqrt(var + norm_eps)[:, None] * final_gain[None, :]
    ).astype(jnp.bfloat16)


MESH = pl.DeviceIdType.MESH
LANES = 128
PAD = 16
CHUNKS = 4
F32 = jnp.float32
BF16 = jnp.bfloat16


def layer_kernel(
    n,
    n_tp,
    key_ref,
    val_ref,
    aux_ref,
    sink_ref,
    query_ref,
    out_proj_ref,
    residual_ref,
    mix_ref,
    gate_ref,
    value_ref,
    down_ref,
    final_ref,
    out_ref,
    gate_all,
    value_all,
    down_all,
    key_ext,
    val_ext,
    docs_ext,
    docs_other,
    doc_cols,
    mask_cols,
    taps_all,
    queries,
    proj,
    rest,
    heads,
    parts,
    parts_in,
    norm_own,
    norm_cols,
    normed,
    up_gate,
    up_value,
    hidden,
    terms,
    terms_in,
    second,
    stats,
    plane_send,
    row_send,
    core_send,
    block_recv,
    core_recv,
    local_sem,
    taps_send,
    taps_recv,
    halo_send,
    halo_recv,
    rows_send,
    rows_recv,
    norm_send,
    norm_recv,
    cols_send,
    cols_recv,
    tail_send,
    tail_recv,
    term_send,
    term_recv,
    stat_send,
    stat_recv,
):
    sp = lax.axis_index("sp")
    tp = lax.axis_index("tp")
    rows = query_ref.shape[0]
    ff = gate_ref.shape[1]
    width = residual_ref.shape[1]
    depth = gate_ref.shape[0]
    cols = down_ref.shape[1]
    share = width // n_tp
    per = share // cols
    planes = n // 2
    z, y = sp // 2, lax.rem(sp, 2)
    x, core = tp // 2, lax.rem(tp, 2)
    low = lax.rem(z, 2)
    half = z // 2
    inner = lax.rem(low + half, 2) == 1
    home = low == core
    base = sp - 2 * low
    work = base + 2 * core
    unit = 2 * x + low
    partner = base + 2 * (1 - low)
    sibling = 2 * x + 1 - core
    facing = 2 * (1 - x) + core
    across = 2 * z + 1 - y
    after = lax.rem(sp + 1, n)
    peers = [lax.rem(tp + i, n_tp) for i in range(1, n_tp)]
    everyone = n * n_tp
    me = sp * n_tp + tp
    row_share = rows // n_tp

    barrier = pltpu.get_barrier_semaphore()

    def greet(i, carry):
        other = lax.rem(me + i, everyone)
        pl.semaphore_signal(
            barrier,
            inc=1,
            device_id=(other // n_tp, lax.rem(other, n_tp)),
            device_id_type=MESH,
        )
        return carry

    lax.fori_loop(1, everyone, greet, 0)
    docs_ref = aux_ref.at[:, pl.ds(ff, rows)]
    fetch = [
        pltpu.make_async_copy(key_ref, key_ext.at[pl.ds(WIN, rows)], local_sem.at[0]),
        pltpu.make_async_copy(val_ref, val_ext.at[pl.ds(WIN, rows)], local_sem.at[1]),
        pltpu.make_async_copy(docs_ref, docs_ext.at[:, pl.ds(WIN, rows)], local_sem.at[2]),
        pltpu.make_async_copy(query_ref, queries, local_sem.at[3]),
        pltpu.make_async_copy(out_proj_ref, proj, local_sem.at[4]),
        pltpu.make_async_copy(
            residual_ref.at[pl.ds(pl.multiple_of(tp * row_share, row_share), row_share)],
            rest,
            local_sem.at[5],
        ),
    ]
    for copy in fetch:
        copy.start()
    pl.semaphore_wait(barrier, everyone - 1)

    whole = (gate_all, value_all, down_all)
    own = (gate_ref, value_ref, down_ref)
    sizes = (depth // CHUNKS, depth // CHUNKS, ff // CHUNKS)

    def piece(w, q):
        return own[w].at[pl.ds(q * sizes[w], sizes[w])]

    def slot(w, index, q):
        if w == 2:
            return down_all.at[index, pl.ds(q * sizes[2], sizes[2])]
        return whole[w].at[
            pl.ds(pl.multiple_of(index * depth + q * sizes[w], sizes[w]), sizes[w])
        ]

    def slab(w, index):
        if w == 2:
            return down_all.at[index]
        return whole[w].at[pl.ds(pl.multiple_of(index * depth, depth), depth)]

    def to_plane(w, i, q):
        return pltpu.make_async_remote_copy(
            src_ref=piece(w, q),
            dst_ref=slot(w, sp, q),
            send_sem=plane_send.at[w, i, q],
            recv_sem=block_recv.at[w, sp, q],
            device_id=(2 * (core + 2 * i) + y, tp),
            device_id_type=MESH,
        )

    def to_row(w, at, q, source):
        return pltpu.make_async_remote_copy(
            src_ref=source,
            dst_ref=slot(w, 2 * at + y, q),
            send_sem=row_send.at[w, at, q],
            recv_sem=block_recv.at[w, 2 * at + y, q],
            device_id=(across, tp),
            device_id_type=MESH,
        )

    def to_core(w, index, q, source):
        return pltpu.make_async_remote_copy(
            src_ref=source,
            dst_ref=slot(w, index, q),
            send_sem=core_send.at[w, index, q],
            recv_sem=core_recv.at[w, index, q],
            device_id=(sp, sibling),
            device_id_type=MESH,
        )

    def await_piece(w, index, q):
        pltpu.make_async_remote_copy(
            src_ref=slot(w, index, q),
            dst_ref=slot(w, index, q),
            send_sem=core_send.at[w, index, q],
            recv_sem=block_recv.at[w, index, q],
            device_id=(sp, sibling),
            device_id_type=MESH,
        ).wait_recv()

    def near_sends(w):
        for i in range(2):
            @pl.when((half == i) & (core + 2 * i != z))
            def _():
                for q in range(CHUNKS):
                    to_plane(w, i, q).start()

    def far_sends(w, cond):
        for i in range(2):
            @pl.when((half != i) & cond)
            def _():
                for q in range(CHUNKS):
                    to_plane(w, i, q).start()

    def zone(k):
        block = lax.rem(half + k // 2, 2)
        side = low if k < 2 else half
        return 2 * block + lax.rem(side + k % 2, 2)

    def own_row(w):
        @pl.when(home)
        def _():
            for q in range(CHUNKS):
                to_row(w, z, q, piece(w, q)).start()

    def own_core(w):
        @pl.when(home)
        def _():
            for q in range(CHUNKS):
                to_core(w, sp, q, piece(w, q)).start()

    def col(w, k, q):
        at = zone(k)
        index = 2 * at + y
        await_piece(w, index, q)
        to_row(w, at, q, slot(w, index, q)).start()
        to_core(w, index, q, slot(w, index, q)).start()

    def row(w, k, q):
        index = 2 * zone(k) + 1 - y
        await_piece(w, index, q)
        to_core(w, index, q, slot(w, index, q)).start()

    halo = [
        pltpu.make_async_remote_copy(
            src_ref=source,
            dst_ref=target,
            send_sem=halo_send.at[i],
            recv_sem=halo_recv.at[i],
            device_id=(after, tp),
            device_id_type=MESH,
        )
        for i, (source, target) in enumerate(
            (
                (key_ref.at[pl.ds(rows - WIN, WIN)], key_ext.at[pl.ds(0, WIN)]),
                (val_ref.at[pl.ds(rows - WIN, WIN)], val_ext.at[pl.ds(0, WIN)]),
                (
                    aux_ref.at[:, pl.ds(ff + rows - WIN, WIN)],
                    docs_ext.at[:, pl.ds(0, WIN)],
                ),
            )
        )
    ]
    for copy in halo:
        copy.start()
    near_sends(0)
    far_sends(0, True)
    own_row(0)
    own_row(1)
    near_sends(1)
    far_sends(1, inner)
    settle = [
        pltpu.make_async_copy(own[w], slab(w, sp), local_sem.at[6 + w]) for w in range(3)
    ]
    settle.append(
        pltpu.make_async_copy(aux_ref.at[:, pl.ds(0, ff)], taps_all, local_sem.at[9])
    )
    taps_copy = pltpu.make_async_remote_copy(
        src_ref=aux_ref.at[:, pl.ds(0, ff)],
        dst_ref=taps_all,
        send_sem=taps_send,
        recv_sem=taps_recv,
        device_id=(sp, sibling),
        device_id_type=MESH,
    )

    @pl.when(home)
    def _():
        for copy in settle:
            copy.start()
        taps_copy.start()

    own_core(0)
    own_core(1)
    for copy in fetch:
        copy.wait()

    line = lax.broadcasted_iota(jnp.int32, (LANES, LANES), 0)
    lane = lax.broadcasted_iota(jnp.int32, (LANES, LANES), 1)
    for b in range(1, rows // LANES + 1):
        row_doc = docs_ext[0:1, b * LANES : (b + 1) * LANES]
        doc_cols[b * LANES : (b + 1) * LANES, :] = jnp.broadcast_to(row_doc, (LANES, LANES)).T

    zero = jnp.zeros((2 * WIN, HD), BF16)

    def pair_copy(i, block):
        return pltpu.make_async_remote_copy(
            src_ref=parts.at[block],
            dst_ref=parts_in.at[i],
            send_sem=rows_send.at[i],
            recv_sem=rows_recv.at[i],
            device_id=(sp, sibling),
            device_id_type=MESH,
        )

    def facing_copy():
        return pltpu.make_async_remote_copy(
            src_ref=parts.at[facing],
            dst_ref=parts_in.at[2],
            send_sem=rows_send.at[2],
            recv_sem=rows_recv.at[2],
            device_id=(sp, facing),
            device_id_type=MESH,
        )

    def attend_block(j, carry):
        b = 2 * lax.rem(x + 1 + j, 2) + lax.rem(core + 1 + j // 2, 2)

        @pl.when(b == 0)
        def _():
            for copy in halo:
                copy.wait_recv()

        start = pl.multiple_of(b * WIN, WIN)
        k = key_ext[pl.ds(start, 2 * WIN), :]
        v = val_ext[pl.ds(start, 2 * WIN), :]
        keys = jnp.concatenate(
            [jnp.concatenate([k, zero], axis=1), jnp.concatenate([zero, k], axis=1)], axis=0
        )
        values = jnp.concatenate(
            [jnp.concatenate([v, zero], axis=1), jnp.concatenate([zero, v], axis=1)], axis=0
        )
        query_doc = doc_cols[pl.ds(start + WIN, WIN), :]
        prev_doc = docs_ext[0:1, pl.ds(start, WIN)]
        this_doc = docs_ext[0:1, pl.ds(start + WIN, WIN)]
        prev_ok = (query_doc == prev_doc) & (lane > line) & (sp * rows + b * WIN > 0)
        this_ok = (query_doc == this_doc) & (lane <= line)
        bias = jnp.concatenate(
            [jnp.where(prev_ok, 0.0, -1e30), jnp.where(this_ok, 0.0, -1e30)], axis=1
        ).astype(F32)
        for pair in range(query_ref.shape[1] // LANES):
            block = queries[pl.ds(start, WIN), pair * LANES : (pair + 1) * LANES]
            both = lax.dot_general(
                block, keys, (((1,), (1,)), ((), ())), preferred_element_type=F32
            )
            probs = []
            for side in (0, 1):
                scores = both[:, side * 2 * WIN : (side + 1) * 2 * WIN] * HD ** (-0.5) + bias
                sink = sink_ref[2 * pair + side]
                top = jnp.maximum(jnp.max(scores, axis=1, keepdims=True), sink)
                weights = jnp.exp(scores - top)
                total = jnp.sum(weights, axis=1, keepdims=True) + jnp.exp(sink - top)
                probs.append((weights / total).astype(BF16))
            heads[:, pair * LANES : (pair + 1) * LANES] = jnp.dot(
                jnp.concatenate(probs, axis=1), values, preferred_element_type=F32
            ).astype(BF16)
        for c in range(width // 512):
            parts[b, :, c * 512 : (c + 1) * 512] = jnp.dot(
                heads[...], proj[:, c * 512 : (c + 1) * 512], preferred_element_type=F32
            ).astype(BF16)

        @pl.when(j == 0)
        def _():
            pair_copy(0, 2 * (1 - x) + 1 - core).start()

        @pl.when(j == 1)
        def _():
            pair_copy(1, sibling).start()

        @pl.when(j == 2)
        def _():
            pair_copy(0, facing).wait_recv()
            parts[facing] = (parts[facing].astype(F32) + parts_in[0].astype(F32)).astype(BF16)
            facing_copy().start()

        return carry

    lax.fori_loop(0, n_tp, attend_block, 0)

    @pl.when(home)
    def _():
        for q in range(CHUNKS):
            col(0, 1, q)
        for q in range(CHUNKS):
            row(0, 0, q)
        for q in range(CHUNKS):
            row(1, 0, q)

    own_row(2)
    own_core(2)
    pair_copy(1, tp).wait_recv()
    facing_copy().wait_recv()
    first = mix_scale * rest[...].astype(F32) + parts[tp].astype(F32)
    first = first + parts_in[1].astype(F32) + parts_in[2].astype(F32)
    mean = jnp.mean(first, axis=1, keepdims=True)
    first = first - mean
    var = jnp.mean(first * first, axis=1, keepdims=True)
    norm_own[...] = (first * lax.rsqrt(var + norm_eps) * mix_ref[...]).astype(BF16)

    def workers(block):
        parity = lax.rem(block // 2, 2)
        return [
            (block - 2 * parity + 2 * a, 2 * b + parity)
            for a in (0, 1)
            for b in range(n_tp // 2)
        ]

    def place_of(source):
        return pl.ds(pl.multiple_of(PAD + source * row_share, PAD), row_share)

    def norm_copy(i, device, source):
        return pltpu.make_async_remote_copy(
            src_ref=norm_own,
            dst_ref=normed.at[place_of(source)],
            send_sem=norm_send.at[i],
            recv_sem=norm_recv.at[source],
            device_id=device,
            device_id_type=MESH,
        )

    def is_me(device):
        return (device[0] == sp) & (device[1] == tp)

    def cols_copy(i, peer, source):
        rows_at = pl.ds(pl.multiple_of(source * row_share, row_share), row_share)
        return pltpu.make_async_remote_copy(
            src_ref=norm_own.at[:, pl.ds(pl.multiple_of(peer * share, share), share)],
            dst_ref=norm_cols.at[rows_at],
            send_sem=cols_send.at[i],
            recv_sem=cols_recv.at[source],
            device_id=(sp, peer),
            device_id_type=MESH,
        )

    def tail_copy(i, device):
        return pltpu.make_async_remote_copy(
            src_ref=norm_own.at[pl.ds(row_share - PAD, PAD)],
            dst_ref=normed.at[pl.ds(0, PAD)],
            send_sem=tail_send.at[i],
            recv_sem=tail_recv,
            device_id=device,
            device_id_type=MESH,
        )

    own_workers = workers(sp)
    next_workers = workers(after)

    @pl.when(tp == n_tp - 1)
    def _():
        for i, device in enumerate(next_workers):
            tail_copy(i, device).start()

    for i, device in enumerate(own_workers):
        @pl.when(jnp.logical_not(is_me(device)))
        def _():
            norm_copy(i, device, tp).start()

    far_sends(1, jnp.logical_not(inner))
    near_sends(2)
    far_sends(2, True)
    for i, peer in enumerate(peers):
        cols_copy(i, peer, tp).start()

    docs_copy = pltpu.make_async_remote_copy(
        src_ref=docs_ext,
        dst_ref=docs_other,
        send_sem=halo_send.at[3],
        recv_sem=halo_recv.at[3],
        device_id=(partner, tp),
        device_id_type=MESH,
    )
    docs_copy.start()

    @pl.when(home)
    def _():
        normed[place_of(tp), :] = norm_own[...]

    norm_cols[pl.ds(pl.multiple_of(tp * row_share, row_share), row_share), :] = norm_own[
        :, pl.ds(pl.multiple_of(tp * share, share), share)
    ]

    @pl.when(home)
    def _():
        for q in range(CHUNKS):
            col(0, 2, q)
            col(0, 3, q)
        for q in range(CHUNKS):
            col(1, 1, q)
        for q in range(CHUNKS):
            row(0, 1, q)
        for q in range(CHUNKS):
            col(1, 2, q)
            row(0, 2, q)
            row(0, 3, q)
        for q in range(CHUNKS):
            row(1, 1, q)
        for q in range(CHUNKS):
            col(1, 3, q)
        for q in range(CHUNKS):
            col(2, 1, q)
        for q in range(CHUNKS):
            row(1, 2, q)
            row(1, 3, q)

    docs_copy.wait_recv()
    place = lax.broadcasted_iota(jnp.int32, (LANES, LANES), 0)
    for b in range(rows // LANES):
        def columns(lag):
            at = pl.ds(WIN + b * LANES - lag, LANES)
            return at

        now = slice(WIN + b * LANES, WIN + (b + 1) * LANES)
        before = slice(b * LANES, (b + 1) * LANES)
        doc_now = jnp.where(home, docs_ext[0:1, now], docs_other[0:1, now])
        doc_before = jnp.where(home, docs_ext[0:1, before], docs_other[0:1, before])
        tall = jnp.broadcast_to(doc_now, (LANES, LANES)).T
        ahead = jnp.broadcast_to(doc_before, (LANES, LANES)).T
        mask_cols[0, PAD + b * LANES : PAD + (b + 1) * LANES, :] = tall
        if b == 0:
            mask_cols[0, 0:PAD, :] = ahead[LANES - PAD :]
    for b in range(rows // LANES):
        at = PAD + b * LANES
        doc = mask_cols[0, at : at + LANES, :]
        for lag in range(1, TAPS):
            same = (mask_cols[0, at - lag : at - lag + LANES, :] == doc) & (
                place + (work * rows + b * LANES) >= lag
            )
            mask_cols[lag, at : at + LANES, :] = jnp.where(same, 1.0, 0.0).astype(F32)

    for source in range(n_tp):
        @pl.when(jnp.logical_not(home & (tp == source)))
        def _():
            norm_copy(0, (sp, sibling), source).wait_recv()

    tail_copy(0, (sp, sibling)).wait_recv()

    def await_core(w, index):
        for q in range(CHUNKS):
            to_core(w, index, q, slot(w, index, q)).wait_recv()

    @pl.when(home)
    def _():
        for copy in settle:
            copy.wait()

    @pl.when(jnp.logical_not(home))
    def _():
        taps_copy.wait_recv()

        def await_both(index, carry):
            for w in (0, 1):
                await_core(w, index)
            return carry

        lax.fori_loop(0, n, await_both, 0)

    def convolved(source, first_tap, at):
        total = taps_all[first_tap : first_tap + 1, pl.ds(at, LANES)] * source[PAD : PAD + rows, :]
        for lag in range(1, TAPS):
            tap = taps_all[first_tap + lag : first_tap + lag + 1, pl.ds(at, LANES)]
            shifted = source[PAD - lag : PAD - lag + rows, :]
            total = total + tap * (shifted * mask_cols[lag, PAD : PAD + rows, :])
        return total

    def up_block(c, carry):
        at = pl.multiple_of(c * LANES, LANES)
        weights = jnp.concatenate(
            [gate_all[:, pl.ds(at, LANES)], value_all[:, pl.ds(at, LANES)]], axis=1
        )
        both = jnp.dot(normed[...], weights, preferred_element_type=F32)
        both = both.astype(BF16).astype(F32)
        up_gate[...] = both[:, :LANES]
        up_value[...] = both[:, LANES:]
        gate = convolved(up_gate, 0, at)
        value = convolved(up_value, TAPS, at)
        inside = math.sqrt(2.0 / math.pi) * (gate + 0.044715 * (gate * gate * gate))
        hidden[:, pl.ds(at, LANES)] = (0.5 * gate * (1.0 + jnp.tanh(inside)) * value).astype(BF16)
        for q in range(CHUNKS):
            @pl.when(home & (c == 2 * q + 1))
            def _():
                row(2, 0, q)

        return carry

    lax.fori_loop(0, ff // LANES, up_block, 0)

    def term_copy(index, source):
        owner = index // per
        return pltpu.make_async_remote_copy(
            src_ref=terms.at[index],
            dst_ref=terms_in.at[source, lax.rem(index, per)],
            send_sem=term_send.at[index],
            recv_sem=term_recv.at[source, lax.rem(index, per)],
            device_id=(work, owner),
            device_id_type=MESH,
        )

    def down_block(k, flip):
        index = 2 * zone(k) + (1 - y if flip else y)

        @pl.when(home)
        def _():
            if k > 0 and not flip and k > 1:
                for q in range(CHUNKS):
                    col(2, k, q)
            if k > 0 and flip:
                for q in range(CHUNKS):
                    row(2, k, q)

        @pl.when(jnp.logical_not(home))
        def _():
            await_core(2, index)

        terms[index] = jnp.dot(
            hidden[...], down_all[index], preferred_element_type=F32
        ).astype(BF16)

        mine = home & (index // per == tp)

        @pl.when(mine)
        def _():
            terms_in[tp, lax.rem(index, per)] = terms[index]

        @pl.when(jnp.logical_not(mine))
        def _():
            term_copy(index, unit).start()

    for k, flip in ((0, 0), (0, 1), (1, 0), (1, 1), (2, 0), (3, 0), (2, 1), (3, 1)):
        down_block(k, flip)

    for source in range(n_tp):
        @pl.when(jnp.logical_not(home & (tp == source)))
        def _():
            for j in range(per):
                pltpu.make_async_remote_copy(
                    src_ref=terms_in.at[source, j],
                    dst_ref=terms_in.at[source, j],
                    send_sem=term_send.at[0],
                    recv_sem=term_recv.at[source, j],
                    device_id=(sp, sibling),
                    device_id_type=MESH,
                ).wait_recv()

    for i, peer in enumerate(peers):
        cols_copy(i, peer, peer).wait_recv()

    sums = jnp.zeros((rows, 1), F32)
    squares = jnp.zeros((rows, 1), F32)
    for j in range(per):
        total = mix_scale * norm_cols[:, j * cols : (j + 1) * cols].astype(F32)
        for source in range(n_tp):
            total = total + terms_in[source, j].astype(F32)
        second[:, j * cols : (j + 1) * cols] = total
        sums = sums + jnp.sum(total, axis=1, keepdims=True)
        squares = squares + jnp.sum(total * total, axis=1, keepdims=True)
    which = lax.broadcasted_iota(jnp.int32, (rows, LANES), 1)
    packed = jnp.where(which == 0, sums, jnp.where(which == 1, squares, 0.0))
    stats[tp] = packed.T[0:8]

    def stat_copy(peer, source):
        return pltpu.make_async_remote_copy(
            src_ref=stats.at[source],
            dst_ref=stats.at[source],
            send_sem=stat_send.at[peer],
            recv_sem=stat_recv.at[source],
            device_id=(sp, peer),
            device_id_type=MESH,
        )

    for peer in peers:
        stat_copy(peer, tp).start()

    for w in range(3):
        for i in range(2):
            @pl.when(core + 2 * i != z)
            def _():
                for q in range(CHUNKS):
                    to_plane(w, i, q).wait_send()

    @pl.when(home)
    def _():
        def drain(index, carry):
            for w in range(3):
                for q in range(CHUNKS):
                    to_core(w, index, q, slot(w, index, q)).wait_send()
            return carry

        lax.fori_loop(0, n, drain, 0)

        def drain_rows(at, carry):
            for w in range(3):
                for q in range(CHUNKS):
                    to_row(w, at, q, slot(w, 2 * at + y, q)).wait_send()
            return carry

        lax.fori_loop(0, planes, drain_rows, 0)
        taps_copy.wait_send()

    for copy in halo:
        copy.wait_send()
    docs_copy.wait_send()
    for i, device in enumerate(own_workers):
        @pl.when(jnp.logical_not(is_me(device)))
        def _():
            norm_copy(i, device, tp).wait_send()

    @pl.when(tp == n_tp - 1)
    def _():
        for i, device in enumerate(next_workers):
            tail_copy(i, device).wait_send()

    pair_copy(0, 2 * (1 - x) + 1 - core).wait_send()
    pair_copy(1, sibling).wait_send()
    facing_copy().wait_send()
    for i, peer in enumerate(peers):
        cols_copy(i, peer, tp).wait_send()
    for index in range(n):
        @pl.when(jnp.logical_not(home & (tp == index // per)))
        def _():
            term_copy(index, unit).wait_send()

    for peer in peers:
        stat_copy(peer, peer).wait_recv()
    total = stats[0]
    for source in range(1, n_tp):
        total = total + stats[source]
    spread = jnp.concatenate([total] * (LANES // 8), axis=0).T
    mean = spread[:, 0:1] / width
    var = spread[:, 1:2] / width - mean * mean
    out_ref[...] = (
        (second[...] - mean) * lax.rsqrt(var + norm_eps) * final_ref[...]
    ).astype(BF16)
    for peer in peers:
        stat_copy(peer, tp).wait_send()


def fused(
    query_rows,
    key_rows,
    value_rows,
    doc_ids,
    sink_logit,
    residual,
    out_proj,
    mix_gain,
    gate_proj,
    value_proj,
    gate_taps,
    value_taps,
    down_proj,
    final_gain,
):
    n = lax.axis_size("sp")
    n_tp = lax.axis_size("tp")
    rows, head_cols = query_rows.shape
    width = residual.shape[1]
    depth, ff = gate_proj.shape
    cols = down_proj.shape[1]
    per = width // n_tp // cols
    planes = n // 2
    taps = jnp.concatenate(
        [gate_taps, value_taps, jnp.zeros((8 - 2 * TAPS, ff), F32)], axis=0
    )
    docs = jnp.broadcast_to(doc_ids.astype(F32)[None, :], (8, rows))
    aux = jnp.concatenate([taps, docs], axis=1)
    share = rows // n_tp
    anywhere = pl.BlockSpec(memory_space=pl.ANY)
    vmem = pl.BlockSpec(memory_space=pltpu.VMEM)
    smem = pl.BlockSpec(memory_space=pltpu.SMEM)
    dma = pltpu.SemaphoreType.DMA
    return pl.pallas_call(
        functools.partial(layer_kernel, n, n_tp),
        out_shape=jax.ShapeDtypeStruct((rows, width // n_tp), BF16),
        in_specs=[
            anywhere, anywhere, anywhere, smem, anywhere, anywhere, anywhere, vmem,
            anywhere, anywhere, anywhere, vmem,
        ],
        out_specs=vmem,
        scratch_shapes=[
            pltpu.VMEM((n * depth, ff), BF16),
            pltpu.VMEM((n * depth, ff), BF16),
            pltpu.VMEM((n, ff, cols), BF16),
            pltpu.VMEM((WIN + rows, HD), BF16),
            pltpu.VMEM((WIN + rows, HD), BF16),
            pltpu.VMEM((8, WIN + rows), F32),
            pltpu.VMEM((8, WIN + rows), F32),
            pltpu.VMEM((WIN + rows, LANES), F32),
            pltpu.VMEM((TAPS, PAD + rows, LANES), F32),
            pltpu.VMEM((8, ff), F32),
            pltpu.VMEM((rows, head_cols), BF16),
            pltpu.VMEM((head_cols, width), BF16),
            pltpu.VMEM((share, width), BF16),
            pltpu.VMEM((share, head_cols), BF16),
            pltpu.VMEM((n_tp, share, width), BF16),
            pltpu.VMEM((3, share, width), BF16),
            pltpu.VMEM((share, width), BF16),
            pltpu.VMEM((rows, width // n_tp), BF16),
            pltpu.VMEM((PAD + rows, width), BF16),
            pltpu.VMEM((PAD + rows, LANES), F32),
            pltpu.VMEM((PAD + rows, LANES), F32),
            pltpu.VMEM((rows, ff), BF16),
            pltpu.VMEM((n, rows, cols), BF16),
            pltpu.VMEM((n_tp, per, rows, cols), BF16),
            pltpu.VMEM((rows, width // n_tp), F32),
            pltpu.VMEM((n_tp, 8, rows), F32),
            dma((3, 2, CHUNKS)),
            dma((3, planes, CHUNKS)),
            dma((3, n, CHUNKS)),
            dma((3, n, CHUNKS)),
            dma((3, n, CHUNKS)),
            dma((10,)),
            dma(()),
            dma(()),
            dma((4,)),
            dma((4,)),
            dma((3,)),
            dma((3,)),
            dma((n_tp,)),
            dma((n_tp,)),
            dma((n_tp,)),
            dma((n_tp,)),
            dma((n_tp,)),
            dma(()),
            dma((n,)),
            dma((n_tp, per)),
            dma((n_tp,)),
            dma((n_tp,)),
        ],
        compiler_params=pltpu.CompilerParams(
            collective_id=0, has_side_effects=True, vmem_limit_bytes=60 * 1024 * 1024
        ),
        name="layer",
    )(
        key_rows,
        value_rows,
        aux,
        sink_logit,
        query_rows,
        out_proj,
        residual,
        mix_gain[None, :],
        gate_proj,
        value_proj,
        down_proj,
        final_gain[None, :],
    )


def on_any(*args):
    query_rows, key_rows, gate_proj, down_proj = args[0], args[1], args[8], args[12]
    n, n_tp = lax.axis_size("sp"), lax.axis_size("tp")
    share = args[5].shape[1] // n_tp
    depth, ff = gate_proj.shape
    cols = down_proj.shape[1]
    fits = (
        n == 8
        and n_tp == 4
        and ff >= 10 * LANES
        and query_rows.shape[0] == n_tp * WIN
        and key_rows.shape[1] == HD
        and query_rows.shape[1] % LANES == 0
        and depth % (16 * CHUNKS) == 0
        and ff % LANES == 0
        and ff % (16 * CHUNKS) == 0
        and cols % LANES == 0
        and share % cols == 0
    )
    return fused(*args) if fits else on_device(*args)


def solution(mesh):
    placed = (
        P("sp", "tp"),
        P("sp", "tp"),
        P("sp", "tp"),
        P("sp"),
        P("tp"),
        P("sp", None),
        P("tp", None),
        P(),
        P("sp", "tp"),
        P("sp", "tp"),
        P(None, "tp"),
        P(None, "tp"),
        P("tp", "sp"),
        P("tp"),
    )
    return jax.shard_map(
        on_any, mesh=mesh, in_specs=placed, out_specs=P("sp", "tp"), check_vma=False
    )
```

```python
import functools
import math

import jax
import jax.numpy as jnp
from jax import lax
from jax.experimental import pallas as pl
from jax.experimental.pallas import tpu as pltpu
from jax.sharding import PartitionSpec as P

HD = 64
WIN = 128
TAPS = 3


mix_scale = math.sqrt(2.0)
norm_eps = 1e-05


def passed_along(block, axis, distance):
    devices = range(lax.axis_size(axis))
    route = [(i - distance, i) for i in devices if i - distance in devices]
    return lax.ppermute(block, axis, route)


def attend(query_block, key_block, value_block, query_pos, key_pos, query_doc, key_doc, sink):
    head_size = query_block.shape[-1]
    scores = jnp.einsum(
        "qkgd,skd->kgqs", query_block, key_block, preferred_element_type=jnp.float32
    ) * head_size ** (-0.5)
    diff = query_pos[:, None] - key_pos[None, :]
    valid = (
        (diff >= 0)
        & (diff < WIN)
        & (query_doc[:, None] == key_doc[None, :])
        & (key_pos[None, :] >= 0)
    )
    scores = jnp.where(valid[None, None], scores, -1e30)
    top = jnp.maximum(jnp.max(scores, axis=-1, keepdims=True), sink)
    weights = jnp.exp(scores - top)
    total = jnp.sum(weights, axis=-1, keepdims=True) + jnp.exp(sink - top)
    probs = (weights / total).astype(jnp.bfloat16)
    out = jnp.einsum("kgqs,skd->qkgd", probs, value_block, preferred_element_type=jnp.float32)
    return out.astype(jnp.bfloat16)


def depthwise(tail, current, taps, tail_docs, docs):
    extended = jnp.concatenate([tail, current])
    ext_docs = jnp.concatenate([tail_docs, docs])
    lag_rows = tail.shape[0]
    count = current.shape[0]
    total = jnp.zeros(current.shape, jnp.float32)
    for lag in range(lag_rows + 1):
        start = lag_rows - lag
        same = (ext_docs[start : start + count] == docs)[:, None]
        rows = extended[start : start + count].astype(jnp.float32)
        total = total + taps[lag][None, :] * jnp.where(same, rows, 0.0)
    return total


def on_device(
    query_rows,
    key_rows,
    value_rows,
    doc_ids,
    sink_logit,
    residual,
    out_proj,
    mix_gain,
    gate_proj,
    value_proj,
    gate_taps,
    value_taps,
    down_proj,
    final_gain,
):
    rows = query_rows.shape[0]
    kv_local = key_rows.shape[1] // HD
    heads_local = query_rows.shape[1] // HD
    groups = heads_local // kv_local
    offset = lax.axis_index("sp") * rows
    prev_keys, prev_values, prev_docs = passed_along(
        (key_rows[rows - WIN :], value_rows[rows - WIN :], doc_ids[rows - WIN :]), "sp", 1
    )
    all_keys = jnp.concatenate([prev_keys, key_rows]).reshape(rows + WIN, kv_local, HD)
    all_values = jnp.concatenate([prev_values, value_rows]).reshape(rows + WIN, kv_local, HD)
    all_docs = jnp.concatenate([prev_docs, doc_ids])
    key_pos = offset - WIN + jnp.arange(rows + WIN, dtype=jnp.int32)
    query_pos = offset + jnp.arange(rows, dtype=jnp.int32)
    queries = query_rows.reshape(rows, kv_local, groups, HD)
    sink = sink_logit.reshape(kv_local, groups, 1, 1)
    pieces = attend(queries, all_keys, all_values, query_pos, key_pos, doc_ids, all_docs, sink)
    heads = pieces.reshape(rows, heads_local * HD)
    partial_value = jnp.dot(heads, out_proj, preferred_element_type=jnp.float32)
    width = residual.shape[1]
    share = width // lax.axis_size("tp")
    col_start = lax.axis_index("tp") * share
    attn_total = lax.psum(partial_value.astype(jnp.bfloat16), "tp").astype(jnp.float32)
    first_sum = mix_scale * residual.astype(jnp.float32) + attn_total
    mean = jnp.mean(first_sum, axis=1, keepdims=True)
    var = jnp.mean(jnp.square(first_sum - mean), axis=1, keepdims=True)
    normed = ((first_sum - mean) * lax.rsqrt(var + norm_eps) * mix_gain[None, :]).astype(
        jnp.bfloat16
    )
    normed_own = lax.dynamic_slice_in_dim(normed, col_start, share, 1)
    up_gate = jnp.dot(
        normed,
        lax.all_gather(gate_proj, "sp", axis=0, tiled=True),
        preferred_element_type=jnp.float32,
    )
    up_value = jnp.dot(
        normed,
        lax.all_gather(value_proj, "sp", axis=0, tiled=True),
        preferred_element_type=jnp.float32,
    )
    up_gate = up_gate.astype(jnp.bfloat16)
    up_value = up_value.astype(jnp.bfloat16)
    lag_rows = TAPS - 1
    prev_gate, prev_value = passed_along(
        (up_gate[rows - lag_rows :], up_value[rows - lag_rows :]), "sp", 1
    )
    tail_docs = prev_docs[WIN - lag_rows :]
    conv_gate = depthwise(prev_gate, up_gate, gate_taps, tail_docs, doc_ids)
    conv_value = depthwise(prev_value, up_value, value_taps, tail_docs, doc_ids)
    hidden = (jax.nn.gelu(conv_gate) * conv_value).astype(jnp.bfloat16)
    terms = jnp.dot(
        hidden,
        lax.all_gather(down_proj, "sp", axis=1, tiled=True),
        preferred_element_type=jnp.float32,
    )
    ffn_own = lax.psum_scatter(
        terms.astype(jnp.bfloat16), "tp", scatter_dimension=1, tiled=True
    ).astype(jnp.float32)
    second_sum = mix_scale * normed_own.astype(jnp.float32) + ffn_own
    row_sum, row_squares = lax.psum(
        (jnp.sum(second_sum, axis=1), jnp.sum(second_sum * second_sum, axis=1)), "tp"
    )
    mean = row_sum / width
    var = row_squares / width - mean * mean
    return (
        (second_sum - mean[:, None]) * lax.rsqrt(var + norm_eps)[:, None] * final_gain[None, :]
    ).astype(jnp.bfloat16)


MESH = pl.DeviceIdType.MESH
LANES = 128
PAD = 16
CHUNKS = 4
PAIR = (0, 1)
EARLY = (
    [("col", 0, 1, i) for i in PAIR]
    + [("far", 1, 0, 0)]
    + [("row", 0, 0, i) for i in PAIR]
    + [("row", 1, 0, i) for i in PAIR]
)
MIDDLE = (
    [("col", 1, 1, i) for i in PAIR]
    + [("far", 2, 0, 0)]
    + [("col", 2, 1, i) for i in PAIR]
    + [("row", 2, 0, i) for i in PAIR]
    + [(kind, 0, k, i) for i in PAIR for kind, k in (("col", 2), ("col", 3), ("row", 1))]
    + [("norm", 0, 0, 0)]
    + [("row", 1, 1, i) for i in PAIR]
    + [(kind, w, k, i) for i in PAIR for w, kind, k in ((1, "col", 2), (0, "row", 2), (1, "col", 3), (0, "row", 3))]
    + [("row", 1, k, i) for i in PAIR for k in (2, 3)]
)
UP_SERVE = ((2, [("row", 2, 1, 0)]), (4, [("row", 2, 1, 1)]))
DOWN_SERVE = {
    (2, 0): [("col", 2, 2, i) for i in PAIR],
    (3, 0): [("col", 2, 3, i) for i in PAIR],
    (2, 1): [("row", 2, 2, i) for i in PAIR],
    (3, 1): [("row", 2, 3, i) for i in PAIR],
}
F32 = jnp.float32
BF16 = jnp.bfloat16


def layer_kernel(
    n,
    n_tp,
    key_ref,
    val_ref,
    docs_ref,
    sink_ref,
    query_ref,
    out_proj_ref,
    residual_ref,
    mix_ref,
    gate_ref,
    value_ref,
    gate_taps_ref,
    value_taps_ref,
    down_ref,
    final_ref,
    out_ref,
    gate_all,
    value_all,
    down_all,
    key_ext,
    val_ext,
    docs_ext,
    docs_other,
    doc_cols,
    mask_cols,
    taps_gate,
    taps_value,
    queries,
    proj,
    rest,
    heads,
    parts,
    parts_in,
    norm_own,
    norm_cols,
    normed,
    up_gate,
    up_value,
    hidden,
    terms,
    terms_in,
    second,
    stats,
    plane_send,
    onward_send,
    row_send,
    core_send,
    block_recv,
    core_recv,
    local_sem,
    taps_send,
    taps_recv,
    halo_send,
    halo_recv,
    rows_send,
    rows_recv,
    norm_send,
    norm_recv,
    pass_send,
    cols_send,
    cols_recv,
    tail_send,
    tail_recv,
    term_send,
    term_recv,
    stat_send,
    stat_recv,
):
    sp = lax.axis_index("sp")
    tp = lax.axis_index("tp")
    rows = query_ref.shape[0]
    ff = gate_ref.shape[1]
    width = residual_ref.shape[1]
    depth = gate_ref.shape[0]
    cols = down_ref.shape[1]
    share = width // n_tp
    per = share // cols
    planes = n // 2
    z, y = sp // 2, lax.rem(sp, 2)
    x, core = tp // 2, lax.rem(tp, 2)
    low = lax.rem(z, 2)
    half = z // 2
    inner = lax.rem(low + half, 2) == 1
    home = low == core
    base = sp - 2 * low
    work = base + 2 * core
    unit = 2 * x + low
    partner = base + 2 * (1 - low)
    sibling = 2 * x + 1 - core
    facing = 2 * (1 - x) + core
    across = 2 * z + 1 - y
    after = lax.rem(sp + 1, n)
    peers = [lax.rem(tp + i, n_tp) for i in range(1, n_tp)]
    everyone = n * n_tp
    me = sp * n_tp + tp
    row_share = rows // n_tp

    barrier = pltpu.get_barrier_semaphore()

    def greet(i, carry):
        other = lax.rem(me + i, everyone)
        pl.semaphore_signal(
            barrier,
            inc=1,
            device_id=(other // n_tp, lax.rem(other, n_tp)),
            device_id_type=MESH,
        )
        return carry

    lax.fori_loop(1, everyone, greet, 0)
    fetch = [
        pltpu.make_async_copy(key_ref, key_ext.at[:, pl.ds(WIN, rows)], local_sem.at[0]),
        pltpu.make_async_copy(val_ref, val_ext.at[:, pl.ds(WIN, rows)], local_sem.at[1]),
        pltpu.make_async_copy(docs_ref, docs_ext.at[:, pl.ds(WIN, rows)], local_sem.at[2]),
        pltpu.make_async_copy(query_ref, queries, local_sem.at[3]),
        pltpu.make_async_copy(out_proj_ref, proj, local_sem.at[4]),
        pltpu.make_async_copy(
            residual_ref.at[pl.ds(pl.multiple_of(tp * row_share, row_share), row_share)],
            rest,
            local_sem.at[5],
        ),
    ]
    for copy in fetch:
        copy.start()
    pl.semaphore_wait(barrier, everyone - 1)

    whole = (gate_all, value_all, down_all)
    own = (gate_ref, value_ref, down_ref)
    sizes = (depth // CHUNKS, depth // CHUNKS, ff // CHUNKS)

    def piece(w, q):
        return own[w].at[pl.ds(q * sizes[w], sizes[w])]

    def slot(w, index, q):
        if w == 2:
            return down_all.at[index, pl.ds(q * sizes[2], sizes[2])]
        return whole[w].at[
            pl.ds(pl.multiple_of(index * depth + q * sizes[w], sizes[w]), sizes[w])
        ]

    def slab(w, index):
        if w == 2:
            return down_all.at[index]
        return whole[w].at[pl.ds(pl.multiple_of(index * depth, depth), depth)]

    def to_plane(w, i, q):
        return pltpu.make_async_remote_copy(
            src_ref=piece(w, q),
            dst_ref=slot(w, sp, q),
            send_sem=plane_send.at[w, i, q],
            recv_sem=block_recv.at[w, sp, q],
            device_id=(2 * (core + 2 * i) + y, 2 * x + (core if q % 2 == 0 else 1 - core)),
            device_id_type=MESH,
        )

    def to_row(w, at, q, source, target):
        return pltpu.make_async_remote_copy(
            src_ref=source,
            dst_ref=slot(w, 2 * at + y, q),
            send_sem=row_send.at[w, at, q],
            recv_sem=block_recv.at[w, 2 * at + y, q],
            device_id=(across, target),
            device_id_type=MESH,
        )

    def to_core(w, index, q, source):
        return pltpu.make_async_remote_copy(
            src_ref=source,
            dst_ref=slot(w, index, q),
            send_sem=core_send.at[w, index, q],
            recv_sem=core_recv.at[w, index, q],
            device_id=(sp, sibling),
            device_id_type=MESH,
        )

    def await_piece(w, index, q):
        pltpu.make_async_remote_copy(
            src_ref=slot(w, index, q),
            dst_ref=slot(w, index, q),
            send_sem=core_send.at[w, index, q],
            recv_sem=block_recv.at[w, index, q],
            device_id=(sp, sibling),
            device_id_type=MESH,
        ).wait_recv()

    def near_sends(w):
        for i in range(2):
            @pl.when((half == i) & (core + 2 * i != z))
            def _():
                for q in range(CHUNKS):
                    to_plane(w, i, q).start()

    def far_sends(w, cond):
        for i in range(2):
            @pl.when((half != i) & cond)
            def _():
                for q in range(CHUNKS):
                    to_plane(w, i, q).start()

    def zone(k):
        block = lax.rem(half + k // 2, 2)
        side = low if k < 2 else half
        return 2 * block + lax.rem(side + k % 2, 2)

    def own_row(w):
        @pl.when(home)
        def _():
            for q in range(CHUNKS):
                to_row(w, z, q, piece(w, q), tp if q % 2 == 0 else sibling).start()

    def own_core(w):
        @pl.when(home)
        def _():
            for q in range(CHUNKS):
                to_core(w, sp, q, piece(w, q)).start()

    role = jnp.where(home, 0, 1)

    def onward(w, i):
        index, q = 2 * zone(1) + y, 2 * i + role
        return pltpu.make_async_remote_copy(
            src_ref=slot(w, index, q),
            dst_ref=slot(w, index, q),
            send_sem=onward_send.at[w, i],
            recv_sem=block_recv.at[w, index, q],
            device_id=(2 * (z + 2 - 4 * half) + y, tp),
            device_id_type=MESH,
        )

    def col(w, k, i):
        at, q = zone(k), 2 * i + role
        index = 2 * at + y
        await_piece(w, index, q)
        if k == 1:
            @pl.when(inner)
            def _():
                onward(w, i).start()

        to_row(w, at, q, slot(w, index, q), tp).start()
        to_core(w, index, q, slot(w, index, q)).start()

    def row(w, k, i):
        index, q = 2 * zone(k) + 1 - y, 2 * i + role
        await_piece(w, index, q)
        to_core(w, index, q, slot(w, index, q)).start()

    def serve(events):
        for kind, w, k, i in events:
            if kind == "far":
                far_sends(w, inner)
            elif kind == "norm":
                @pl.when(jnp.logical_not(home))
                def _():
                    for i in PAIR:
                        norm_copy(0, (sp, sibling), 2 * x + i).wait_recv()
                        norm_pass(i).start()

            else:
                (col if kind == "col" else row)(w, k, i)

    def await_slab(w, k, flip):
        index = 2 * zone(k) + (1 - y if flip else y)
        if k == 0 and not flip:
            @pl.when(jnp.logical_not(home))
            def _():
                for q in range(CHUNKS):
                    to_core(w, index, q, slot(w, index, q)).wait_recv()
        else:
            for i in range(CHUNKS // 2):
                q = 2 * i + 1 - role
                to_core(w, index, q, slot(w, index, q)).wait_recv()

    halo = [
        pltpu.make_async_remote_copy(
            src_ref=source,
            dst_ref=target,
            send_sem=halo_send.at[i],
            recv_sem=halo_recv.at[i],
            device_id=(after, tp),
            device_id_type=MESH,
        )
        for i, (source, target) in enumerate(
            (
                (ref.at[:, pl.ds(rows - WIN, WIN)], ext.at[:, pl.ds(0, WIN)])
                for ref, ext in (
                    (key_ref, key_ext),
                    (val_ref, val_ext),
                    (docs_ref, docs_ext),
                )
            )
        )
    ]
    for copy in halo:
        copy.start()
    near_sends(0)
    far_sends(0, inner | home)
    near_sends(1)
    near_sends(2)
    own_row(0)
    own_row(1)
    own_row(2)
    settle = [
        pltpu.make_async_copy(own[w], slab(w, sp), local_sem.at[6 + w]) for w in range(3)
    ]
    tap_pairs = ((gate_taps_ref, taps_gate), (value_taps_ref, taps_value))
    for i, (source, target) in enumerate(tap_pairs):
        settle.append(pltpu.make_async_copy(source, target, local_sem.at[9 + i]))
    taps = [
        pltpu.make_async_remote_copy(
            src_ref=source,
            dst_ref=target,
            send_sem=taps_send.at[i],
            recv_sem=taps_recv.at[i],
            device_id=(sp, sibling),
            device_id_type=MESH,
        )
        for i, (source, target) in enumerate(tap_pairs)
    ]

    @pl.when(home)
    def _():
        for copy in settle + taps:
            copy.start()

    own_core(0)
    own_core(1)
    own_core(2)
    for copy in fetch:
        copy.wait()

    line = lax.broadcasted_iota(jnp.int32, (LANES, LANES), 0)
    lane = lax.broadcasted_iota(jnp.int32, (LANES, LANES), 1)
    for b in range(1, rows // LANES + 1):
        row_doc = docs_ext[0:1, b * LANES : (b + 1) * LANES].astype(F32)
        doc_cols[b * LANES : (b + 1) * LANES, :] = jnp.broadcast_to(row_doc, (LANES, LANES)).T

    zero = jnp.zeros((HD, 2 * WIN), BF16)

    def pair_copy(i, block):
        return pltpu.make_async_remote_copy(
            src_ref=parts.at[block],
            dst_ref=parts_in.at[i],
            send_sem=rows_send.at[i],
            recv_sem=rows_recv.at[i],
            device_id=(sp, sibling),
            device_id_type=MESH,
        )

    def facing_copy():
        return pltpu.make_async_remote_copy(
            src_ref=parts.at[facing],
            dst_ref=parts_in.at[2],
            send_sem=rows_send.at[2],
            recv_sem=rows_recv.at[2],
            device_id=(sp, facing),
            device_id_type=MESH,
        )

    def attend_block(j, carry):
        b = 2 * lax.rem(x + 1 + j, 2) + lax.rem(core + 1 + j // 2, 2)

        @pl.when(b == 0)
        def _():
            for copy in halo:
                copy.wait_recv()

        start = pl.multiple_of(b * WIN, WIN)
        k = key_ext[:, pl.ds(start, 2 * WIN)]
        v = val_ext[:, pl.ds(start, 2 * WIN)]
        keys = jnp.concatenate(
            [jnp.concatenate([k, zero], axis=1), jnp.concatenate([zero, k], axis=1)], axis=0
        )
        values = jnp.concatenate(
            [jnp.concatenate([v, zero], axis=1), jnp.concatenate([zero, v], axis=1)], axis=0
        )
        query_doc = doc_cols[pl.ds(start + WIN, WIN), :]
        prev_doc = docs_ext[0:1, pl.ds(start, WIN)].astype(F32)
        this_doc = docs_ext[0:1, pl.ds(start + WIN, WIN)].astype(F32)
        prev_ok = (query_doc == prev_doc) & (lane > line) & (sp * rows + b * WIN > 0)
        this_ok = (query_doc == this_doc) & (lane <= line)
        bias = jnp.concatenate(
            [jnp.where(prev_ok, 0.0, -1e30), jnp.where(this_ok, 0.0, -1e30)], axis=1
        ).astype(F32)
        for pair in range(query_ref.shape[1] // LANES):
            block = queries[pl.ds(start, WIN), pair * LANES : (pair + 1) * LANES]
            both = jnp.dot(block, keys, preferred_element_type=F32)
            probs = []
            for side in (0, 1):
                scores = both[:, side * 2 * WIN : (side + 1) * 2 * WIN] * HD ** (-0.5) + bias
                sink = sink_ref[2 * pair + side]
                top = jnp.maximum(jnp.max(scores, axis=1, keepdims=True), sink)
                weights = jnp.exp(scores - top)
                total = jnp.sum(weights, axis=1, keepdims=True) + jnp.exp(sink - top)
                probs.append((weights / total).astype(BF16))
            heads[:, pair * LANES : (pair + 1) * LANES] = lax.dot_general(
                jnp.concatenate(probs, axis=1),
                values,
                (((1,), (1,)), ((), ())),
                preferred_element_type=F32,
            ).astype(BF16)
        for c in range(width // 512):
            parts[b, :, c * 512 : (c + 1) * 512] = jnp.dot(
                heads[...], proj[:, c * 512 : (c + 1) * 512], preferred_element_type=F32
            ).astype(BF16)

        @pl.when(j == 0)
        def _():
            pair_copy(0, 2 * (1 - x) + 1 - core).start()

        @pl.when(j == 1)
        def _():
            pair_copy(1, sibling).start()

        @pl.when(j == 2)
        def _():
            pair_copy(0, facing).wait_recv()
            parts[facing] = (parts[facing].astype(F32) + parts_in[0].astype(F32)).astype(BF16)
            facing_copy().start()

        return carry

    lax.fori_loop(0, n_tp, attend_block, 0)

    serve(EARLY)
    pair_copy(1, tp).wait_recv()
    facing_copy().wait_recv()
    first = mix_scale * rest[...].astype(F32) + parts[tp].astype(F32)
    first = first + parts_in[1].astype(F32) + parts_in[2].astype(F32)
    mean = jnp.mean(first, axis=1, keepdims=True)
    first = first - mean
    var = jnp.mean(first * first, axis=1, keepdims=True)
    norm_own[...] = (first * lax.rsqrt(var + norm_eps) * mix_ref[...]).astype(BF16)

    def workers(block):
        parity = lax.rem(block // 2, 2)
        return [
            (block - 2 * parity + 2 * a, 2 * b + parity)
            for a in (0, 1)
            for b in range(n_tp // 2)
        ]

    def place_of(source):
        return pl.ds(pl.multiple_of(PAD + source * row_share, PAD), row_share)

    def norm_copy(i, device, source):
        return pltpu.make_async_remote_copy(
            src_ref=norm_own,
            dst_ref=normed.at[place_of(source)],
            send_sem=norm_send.at[i],
            recv_sem=norm_recv.at[source],
            device_id=device,
            device_id_type=MESH,
        )

    def takes(i, device):
        return jnp.where(device[0] == sp, device[1] != tp, x == i % 2)

    def norm_pass(i):
        return pltpu.make_async_remote_copy(
            src_ref=normed.at[place_of(2 * x + i)],
            dst_ref=normed.at[place_of(2 * x + i)],
            send_sem=pass_send.at[i],
            recv_sem=norm_recv.at[2 * x + i],
            device_id=(sp, facing),
            device_id_type=MESH,
        )

    def cols_copy(i, peer, source):
        rows_at = pl.ds(pl.multiple_of(source * row_share, row_share), row_share)
        return pltpu.make_async_remote_copy(
            src_ref=norm_own.at[:, pl.ds(pl.multiple_of(peer * share, share), share)],
            dst_ref=norm_cols.at[rows_at],
            send_sem=cols_send.at[i],
            recv_sem=cols_recv.at[source],
            device_id=(sp, peer),
            device_id_type=MESH,
        )

    def tail_copy(i, device):
        return pltpu.make_async_remote_copy(
            src_ref=norm_own.at[pl.ds(row_share - PAD // 2, PAD // 2)],
            dst_ref=normed.at[pl.ds(PAD // 2, PAD // 2)],
            send_sem=tail_send.at[i],
            recv_sem=tail_recv,
            device_id=device,
            device_id_type=MESH,
        )

    own_workers = workers(sp)
    next_workers = workers(after)

    @pl.when((tp == n_tp - 1) & (sp < n - 1))
    def _():
        for i, device in enumerate(next_workers):
            tail_copy(i, device).start()

    for i, device in enumerate(own_workers):
        @pl.when(takes(i, device))
        def _():
            norm_copy(i, device, tp).start()

    far_sends(1, home & jnp.logical_not(inner))
    far_sends(2, home & jnp.logical_not(inner))
    for i, peer in enumerate(peers):
        cols_copy(i, peer, tp).start()

    docs_copy = pltpu.make_async_remote_copy(
        src_ref=docs_ext,
        dst_ref=docs_other,
        send_sem=halo_send.at[3],
        recv_sem=halo_recv.at[3],
        device_id=(partner, tp),
        device_id_type=MESH,
    )
    docs_copy.start()

    @pl.when(home)
    def _():
        normed[place_of(tp), :] = norm_own[...]

    norm_cols[pl.ds(pl.multiple_of(tp * row_share, row_share), row_share), :] = norm_own[
        :, pl.ds(pl.multiple_of(tp * share, share), share)
    ]

    serve(MIDDLE)
    docs_copy.wait_recv()
    place = lax.broadcasted_iota(jnp.int32, (LANES, LANES), 0)
    for b in range(rows // LANES):
        now = slice(WIN + b * LANES, WIN + (b + 1) * LANES)
        before = slice(b * LANES, (b + 1) * LANES)
        doc_now = jnp.where(home, docs_ext[0:1, now], docs_other[0:1, now]).astype(F32)
        doc_before = jnp.where(home, docs_ext[0:1, before], docs_other[0:1, before]).astype(F32)
        tall = jnp.broadcast_to(doc_now, (LANES, LANES)).T
        ahead = jnp.broadcast_to(doc_before, (LANES, LANES)).T
        mask_cols[0, PAD + b * LANES : PAD + (b + 1) * LANES, :] = tall
        if b == 0:
            mask_cols[0, 0:PAD, :] = ahead[LANES - PAD :]
    for b in range(rows // LANES):
        at = PAD + b * LANES
        doc = mask_cols[0, at : at + LANES, :]
        for lag in range(1, TAPS):
            same = (mask_cols[0, at - lag : at - lag + LANES, :] == doc) & (
                place + (work * rows + b * LANES) >= lag
            )
            mask_cols[lag, at : at + LANES, :] = jnp.where(same, 1.0, 0.0).astype(F32)

    for source in range(n_tp):
        @pl.when(jnp.where(home, tp != source, x != source // 2))
        def _():
            norm_copy(0, (sp, sibling), source).wait_recv()

    @pl.when(work > 0)
    def _():
        tail_copy(0, (sp, sibling)).wait_recv()

    @pl.when(work == 0)
    def _():
        normed[0:PAD, :] = jnp.zeros((PAD, width), BF16)


    @pl.when(home)
    def _():
        for copy in settle:
            copy.wait()

    @pl.when(jnp.logical_not(home))
    def _():
        for copy in taps:
            copy.wait_recv()

    for w in (0, 1):
        for k in range(planes):
            for flip in (0, 1):
                await_slab(w, k, flip)

    def convolved(source, taps_ref, at):
        total = taps_ref[0:1, pl.ds(at, LANES)] * source[PAD : PAD + rows, :]
        for lag in range(1, TAPS):
            tap = taps_ref[lag : lag + 1, pl.ds(at, LANES)]
            shifted = source[PAD - lag : PAD - lag + rows, :]
            total = total + tap * (shifted * mask_cols[lag, PAD : PAD + rows, :])
        return total

    def up_block(c, carry):
        at = pl.multiple_of(c * LANES, LANES)
        weights = jnp.concatenate(
            [gate_all[:, pl.ds(at, LANES)], value_all[:, pl.ds(at, LANES)]], axis=1
        )
        both = jnp.dot(normed[...], weights, preferred_element_type=F32)
        both = both.astype(BF16).astype(F32)
        up_gate[...] = both[:, :LANES]
        up_value[...] = both[:, LANES:]
        gate = convolved(up_gate, taps_gate, at)
        value = convolved(up_value, taps_value, at)
        inside = math.sqrt(2.0 / math.pi) * (gate + 0.044715 * (gate * gate * gate))
        hidden[:, pl.ds(at, LANES)] = (0.5 * gate * (1.0 + jnp.tanh(inside)) * value).astype(BF16)
        for at_step, events in UP_SERVE:
            @pl.when(c == at_step)
            def _():
                serve(events)

        return carry

    lax.fori_loop(0, ff // LANES, up_block, 0)

    def term_copy(index, source):
        owner = index // per
        return pltpu.make_async_remote_copy(
            src_ref=terms.at[index],
            dst_ref=terms_in.at[source, lax.rem(index, per)],
            send_sem=term_send.at[index],
            recv_sem=term_recv.at[source, lax.rem(index, per)],
            device_id=(work, owner),
            device_id_type=MESH,
        )

    def down_block(k, flip):
        index = 2 * zone(k) + (1 - y if flip else y)

        serve(DOWN_SERVE.get((k, flip), ()))
        await_slab(2, k, flip)
        terms[index] = jnp.dot(
            hidden[...], down_all[index], preferred_element_type=F32
        ).astype(BF16)

        mine = home & (index // per == tp)

        @pl.when(mine)
        def _():
            terms_in[tp, lax.rem(index, per)] = terms[index]

        @pl.when(jnp.logical_not(mine))
        def _():
            term_copy(index, unit).start()

    for k, flip in ((0, 0), (0, 1), (1, 0), (1, 1), (2, 0), (3, 0), (2, 1), (3, 1)):
        down_block(k, flip)

    for source in range(n_tp):
        @pl.when(jnp.logical_not(home & (tp == source)))
        def _():
            for j in range(per):
                pltpu.make_async_remote_copy(
                    src_ref=terms_in.at[source, j],
                    dst_ref=terms_in.at[source, j],
                    send_sem=term_send.at[0],
                    recv_sem=term_recv.at[source, j],
                    device_id=(sp, sibling),
                    device_id_type=MESH,
                ).wait_recv()

    for i, peer in enumerate(peers):
        cols_copy(i, peer, peer).wait_recv()

    sums = jnp.zeros((rows, 1), F32)
    squares = jnp.zeros((rows, 1), F32)
    for j in range(per):
        total = mix_scale * norm_cols[:, j * cols : (j + 1) * cols].astype(F32)
        for source in range(n_tp):
            total = total + terms_in[source, j].astype(F32)
        second[:, j * cols : (j + 1) * cols] = total
        sums = sums + jnp.sum(total, axis=1, keepdims=True)
        squares = squares + jnp.sum(total * total, axis=1, keepdims=True)
    which = lax.broadcasted_iota(jnp.int32, (rows, LANES), 1)
    packed = jnp.where(which == 0, sums, jnp.where(which == 1, squares, 0.0))
    stats[tp] = packed.T[0:8]

    def stat_copy(peer, source):
        return pltpu.make_async_remote_copy(
            src_ref=stats.at[source],
            dst_ref=stats.at[source],
            send_sem=stat_send.at[peer],
            recv_sem=stat_recv.at[source],
            device_id=(sp, peer),
            device_id_type=MESH,
        )

    for peer in peers:
        stat_copy(peer, tp).start()

    for w in range(3):
        for i in range(2):
            @pl.when((core + 2 * i != z) & ((half == i) | inner | home))
            def _():
                for q in range(CHUNKS):
                    to_plane(w, i, q).wait_send()

        @pl.when(inner)
        def _():
            for i in range(CHUNKS // 2):
                onward(w, i).wait_send()

    for k in range(planes):
        at = zone(k)
        for w in range(3):
            for i in range(CHUNKS // 2):
                q = 2 * i + role
                if k > 0:
                    index = 2 * at + y
                    to_row(w, at, q, slot(w, index, q), tp).wait_send()
                    to_core(w, index, q, slot(w, index, q)).wait_send()
                index = 2 * at + 1 - y
                to_core(w, index, q, slot(w, index, q)).wait_send()

    @pl.when(home)
    def _():
        for w in range(3):
            for q in range(CHUNKS):
                to_row(w, z, q, piece(w, q), tp if q % 2 == 0 else sibling).wait_send()
                to_core(w, sp, q, piece(w, q)).wait_send()
        for copy in taps:
            copy.wait_send()

    for copy in halo:
        copy.wait_send()
    docs_copy.wait_send()
    for i, device in enumerate(own_workers):
        @pl.when(takes(i, device))
        def _():
            norm_copy(i, device, tp).wait_send()

    @pl.when(jnp.logical_not(home))
    def _():
        for i in PAIR:
            norm_pass(i).wait_send()

    @pl.when((tp == n_tp - 1) & (sp < n - 1))
    def _():
        for i, device in enumerate(next_workers):
            tail_copy(i, device).wait_send()

    pair_copy(0, 2 * (1 - x) + 1 - core).wait_send()
    pair_copy(1, sibling).wait_send()
    facing_copy().wait_send()
    for i, peer in enumerate(peers):
        cols_copy(i, peer, tp).wait_send()
    for index in range(n):
        @pl.when(jnp.logical_not(home & (tp == index // per)))
        def _():
            term_copy(index, unit).wait_send()

    for peer in peers:
        stat_copy(peer, peer).wait_recv()
    total = stats[0]
    for source in range(1, n_tp):
        total = total + stats[source]
    spread = jnp.concatenate([total] * (LANES // 8), axis=0).T
    mean = spread[:, 0:1] / width
    var = spread[:, 1:2] / width - mean * mean
    out_ref[...] = (
        (second[...] - mean) * lax.rsqrt(var + norm_eps) * final_ref[...]
    ).astype(BF16)
    for peer in peers:
        stat_copy(peer, tp).wait_send()


def fused(
    query_rows,
    key_rows,
    value_rows,
    doc_ids,
    sink_logit,
    residual,
    out_proj,
    mix_gain,
    gate_proj,
    value_proj,
    gate_taps,
    value_taps,
    down_proj,
    final_gain,
):
    n = lax.axis_size("sp")
    n_tp = lax.axis_size("tp")
    rows, head_cols = query_rows.shape
    width = residual.shape[1]
    depth, ff = gate_proj.shape
    cols = down_proj.shape[1]
    per = width // n_tp // cols
    planes = n // 2
    share = rows // n_tp
    anywhere = pl.BlockSpec(memory_space=pl.ANY)
    vmem = pl.BlockSpec(memory_space=pltpu.VMEM)
    smem = pl.BlockSpec(memory_space=pltpu.SMEM)
    dma = pltpu.SemaphoreType.DMA
    return pl.pallas_call(
        functools.partial(layer_kernel, n, n_tp),
        out_shape=jax.ShapeDtypeStruct((rows, width // n_tp), BF16),
        in_specs=[
            anywhere, anywhere, anywhere, smem, anywhere, anywhere, anywhere, vmem,
            anywhere, anywhere, anywhere, anywhere, anywhere, vmem,
        ],
        out_specs=vmem,
        scratch_shapes=[
            pltpu.VMEM((n * depth, ff), BF16),
            pltpu.VMEM((n * depth, ff), BF16),
            pltpu.VMEM((n, ff, cols), BF16),
            pltpu.VMEM((HD, WIN + rows), BF16),
            pltpu.VMEM((HD, WIN + rows), BF16),
            pltpu.VMEM((1, WIN + rows), jnp.int32),
            pltpu.VMEM((1, WIN + rows), jnp.int32),
            pltpu.VMEM((WIN + rows, LANES), F32),
            pltpu.VMEM((TAPS, PAD + rows, LANES), F32),
            pltpu.VMEM(gate_taps.shape, F32),
            pltpu.VMEM(value_taps.shape, F32),
            pltpu.VMEM((rows, head_cols), BF16),
            pltpu.VMEM((head_cols, width), BF16),
            pltpu.VMEM((share, width), BF16),
            pltpu.VMEM((share, head_cols), BF16),
            pltpu.VMEM((n_tp, share, width), BF16),
            pltpu.VMEM((3, share, width), BF16),
            pltpu.VMEM((share, width), BF16),
            pltpu.VMEM((rows, width // n_tp), BF16),
            pltpu.VMEM((PAD + rows, width), BF16),
            pltpu.VMEM((PAD + rows, LANES), F32),
            pltpu.VMEM((PAD + rows, LANES), F32),
            pltpu.VMEM((rows, ff), BF16),
            pltpu.VMEM((n, rows, cols), BF16),
            pltpu.VMEM((n_tp, per, rows, cols), BF16),
            pltpu.VMEM((rows, width // n_tp), F32),
            pltpu.VMEM((n_tp, 8, rows), F32),
            dma((3, 2, CHUNKS)),
            dma((3, CHUNKS // 2)),
            dma((3, planes, CHUNKS)),
            dma((3, n, CHUNKS)),
            dma((3, n, CHUNKS)),
            dma((3, n, CHUNKS)),
            dma((11,)),
            dma((2,)),
            dma((2,)),
            dma((4,)),
            dma((4,)),
            dma((3,)),
            dma((3,)),
            dma((n_tp,)),
            dma((n_tp,)),
            dma((2,)),
            dma((n_tp,)),
            dma((n_tp,)),
            dma((n_tp,)),
            dma(()),
            dma((n,)),
            dma((n_tp, per)),
            dma((n_tp,)),
            dma((n_tp,)),
        ],
        compiler_params=pltpu.CompilerParams(
            collective_id=0, has_side_effects=True, vmem_limit_bytes=60 * 1024 * 1024
        ),
        name="layer",
    )(
        key_rows.T,
        value_rows.T,
        doc_ids[None, :],
        sink_logit,
        query_rows,
        out_proj,
        residual,
        mix_gain[None, :],
        gate_proj,
        value_proj,
        gate_taps,
        value_taps,
        down_proj,
        final_gain[None, :],
    )


def on_any(*args):
    query_rows, key_rows, gate_proj, down_proj = args[0], args[1], args[8], args[12]
    n, n_tp = lax.axis_size("sp"), lax.axis_size("tp")
    share = args[5].shape[1] // n_tp
    depth, ff = gate_proj.shape
    cols = down_proj.shape[1]
    fits = (
        n == 8
        and n_tp == 4
        and ff >= 10 * LANES
        and query_rows.shape[0] == n_tp * WIN
        and key_rows.shape[1] == HD
        and query_rows.shape[1] % LANES == 0
        and depth % (16 * CHUNKS) == 0
        and ff % LANES == 0
        and ff % (16 * CHUNKS) == 0
        and cols % LANES == 0
        and share % cols == 0
    )
    return fused(*args) if fits else on_device(*args)


def solution(mesh):
    placed = (
        P("sp", "tp"),
        P("sp", "tp"),
        P("sp", "tp"),
        P("sp"),
        P("tp"),
        P("sp", None),
        P("tp", None),
        P(),
        P("sp", "tp"),
        P("sp", "tp"),
        P(None, "tp"),
        P(None, "tp"),
        P("tp", "sp"),
        P("tp"),
    )
    return jax.shard_map(
        on_any, mesh=mesh, in_specs=placed, out_specs=P("sp", "tp"), check_vma=False
    )
```

```python
import functools
import math

import jax
import jax.numpy as jnp
from jax import lax
from jax.experimental import pallas as pl
from jax.experimental.pallas import tpu as pltpu
from jax.sharding import PartitionSpec as P

HD = 64
WIN = 128
TAPS = 3


mix_scale = math.sqrt(2.0)
norm_eps = 1e-05


def passed_along(block, axis, distance):
    devices = range(lax.axis_size(axis))
    route = [(i - distance, i) for i in devices if i - distance in devices]
    return lax.ppermute(block, axis, route)


def attend(query_block, key_block, value_block, query_pos, key_pos, query_doc, key_doc, sink):
    head_size = query_block.shape[-1]
    scores = jnp.einsum(
        "qkgd,skd->kgqs", query_block, key_block, preferred_element_type=jnp.float32
    ) * head_size ** (-0.5)
    diff = query_pos[:, None] - key_pos[None, :]
    valid = (
        (diff >= 0)
        & (diff < WIN)
        & (query_doc[:, None] == key_doc[None, :])
        & (key_pos[None, :] >= 0)
    )
    scores = jnp.where(valid[None, None], scores, -1e30)
    top = jnp.maximum(jnp.max(scores, axis=-1, keepdims=True), sink)
    weights = jnp.exp(scores - top)
    total = jnp.sum(weights, axis=-1, keepdims=True) + jnp.exp(sink - top)
    probs = (weights / total).astype(jnp.bfloat16)
    out = jnp.einsum("kgqs,skd->qkgd", probs, value_block, preferred_element_type=jnp.float32)
    return out.astype(jnp.bfloat16)


def depthwise(tail, current, taps, tail_docs, docs):
    extended = jnp.concatenate([tail, current])
    ext_docs = jnp.concatenate([tail_docs, docs])
    lag_rows = tail.shape[0]
    count = current.shape[0]
    total = jnp.zeros(current.shape, jnp.float32)
    for lag in range(lag_rows + 1):
        start = lag_rows - lag
        same = (ext_docs[start : start + count] == docs)[:, None]
        rows = extended[start : start + count].astype(jnp.float32)
        total = total + taps[lag][None, :] * jnp.where(same, rows, 0.0)
    return total


def on_device(
    query_rows,
    key_rows,
    value_rows,
    doc_ids,
    sink_logit,
    residual,
    out_proj,
    mix_gain,
    gate_proj,
    value_proj,
    gate_taps,
    value_taps,
    down_proj,
    final_gain,
):
    rows = query_rows.shape[0]
    kv_local = key_rows.shape[1] // HD
    heads_local = query_rows.shape[1] // HD
    groups = heads_local // kv_local
    offset = lax.axis_index("sp") * rows
    prev_keys, prev_values, prev_docs = passed_along(
        (key_rows[rows - WIN :], value_rows[rows - WIN :], doc_ids[rows - WIN :]), "sp", 1
    )
    all_keys = jnp.concatenate([prev_keys, key_rows]).reshape(rows + WIN, kv_local, HD)
    all_values = jnp.concatenate([prev_values, value_rows]).reshape(rows + WIN, kv_local, HD)
    all_docs = jnp.concatenate([prev_docs, doc_ids])
    key_pos = offset - WIN + jnp.arange(rows + WIN, dtype=jnp.int32)
    query_pos = offset + jnp.arange(rows, dtype=jnp.int32)
    queries = query_rows.reshape(rows, kv_local, groups, HD)
    sink = sink_logit.reshape(kv_local, groups, 1, 1)
    pieces = attend(queries, all_keys, all_values, query_pos, key_pos, doc_ids, all_docs, sink)
    heads = pieces.reshape(rows, heads_local * HD)
    partial_value = jnp.dot(heads, out_proj, preferred_element_type=jnp.float32)
    width = residual.shape[1]
    share = width // lax.axis_size("tp")
    col_start = lax.axis_index("tp") * share
    attn_total = lax.psum(partial_value.astype(jnp.bfloat16), "tp").astype(jnp.float32)
    first_sum = mix_scale * residual.astype(jnp.float32) + attn_total
    mean = jnp.mean(first_sum, axis=1, keepdims=True)
    var = jnp.mean(jnp.square(first_sum - mean), axis=1, keepdims=True)
    normed = ((first_sum - mean) * lax.rsqrt(var + norm_eps) * mix_gain[None, :]).astype(
        jnp.bfloat16
    )
    normed_own = lax.dynamic_slice_in_dim(normed, col_start, share, 1)
    up_gate = jnp.dot(
        normed,
        lax.all_gather(gate_proj, "sp", axis=0, tiled=True),
        preferred_element_type=jnp.float32,
    )
    up_value = jnp.dot(
        normed,
        lax.all_gather(value_proj, "sp", axis=0, tiled=True),
        preferred_element_type=jnp.float32,
    )
    up_gate = up_gate.astype(jnp.bfloat16)
    up_value = up_value.astype(jnp.bfloat16)
    lag_rows = TAPS - 1
    prev_gate, prev_value = passed_along(
        (up_gate[rows - lag_rows :], up_value[rows - lag_rows :]), "sp", 1
    )
    tail_docs = prev_docs[WIN - lag_rows :]
    conv_gate = depthwise(prev_gate, up_gate, gate_taps, tail_docs, doc_ids)
    conv_value = depthwise(prev_value, up_value, value_taps, tail_docs, doc_ids)
    hidden = (jax.nn.gelu(conv_gate) * conv_value).astype(jnp.bfloat16)
    terms = jnp.dot(
        hidden,
        lax.all_gather(down_proj, "sp", axis=1, tiled=True),
        preferred_element_type=jnp.float32,
    )
    ffn_own = lax.psum_scatter(
        terms.astype(jnp.bfloat16), "tp", scatter_dimension=1, tiled=True
    ).astype(jnp.float32)
    second_sum = mix_scale * normed_own.astype(jnp.float32) + ffn_own
    row_sum, row_squares = lax.psum(
        (jnp.sum(second_sum, axis=1), jnp.sum(second_sum * second_sum, axis=1)), "tp"
    )
    mean = row_sum / width
    var = row_squares / width - mean * mean
    return (
        (second_sum - mean[:, None]) * lax.rsqrt(var + norm_eps)[:, None] * final_gain[None, :]
    ).astype(jnp.bfloat16)


MESH = pl.DeviceIdType.MESH
LANES = 128
PAD = 16
CHUNKS = 4
PAIR = (0, 1)
EARLY = (
    [("col", 0, 1, i) for i in PAIR]
    + [("far", 1, 0, 0)]
    + [("row", 0, 0, i) for i in PAIR]
    + [("row", 1, 0, i) for i in PAIR]
)
MIDDLE = (
    [("col", 1, 1, i) for i in PAIR]
    + [("far", 2, 0, 0)]
    + [(kind, 0, k, i) for i in PAIR for kind, k in (("col", 2), ("col", 3), ("row", 1))]
    + [("norm", 0, 0, 0)]
    + [("row", 1, 1, i) for i in PAIR]
    + [(kind, w, k, i) for i in PAIR for w, kind, k in ((1, "col", 2), (0, "row", 2), (1, "col", 3), (0, "row", 3))]
    + [("col", 2, 1, i) for i in PAIR]
    + [("row", 1, k, i) for i in PAIR for k in (2, 3)]
)
UP_SERVE = (
    (0, [("row", 2, 0, i) for i in PAIR]),
    (1, [("row", 2, 1, i) for i in PAIR]),
    (2, [("col", 2, 2, 0)]),
    (3, [("col", 2, 2, 1), ("col", 2, 3, 0)]),
    (4, [("col", 2, 3, 1)]),
)
X_FIRST = ((0, 1), (1, 1))
DOWN_ORDER = (
    ("down", 0, 0),
    ("down", 0, 1),
    ("down", 1, 0),
    ("down", 1, 1),
    ("down", 2, 0),
    ("down", 3, 0),
    ("down", 2, 1),
    ("cross", 2, 0),
    ("down", 3, 1),
    ("cross", 0, 0),
    ("cross", 0, 1),
    ("cross", 1, 0),
    ("cross", 1, 1),
    ("cross", 3, 0),
    ("cross", 2, 1),
    ("cross", 3, 1),
)
DOWN_SERVE = {
    (2, 1): [("row", 2, 2, i) for i in PAIR],
    (3, 1): [("row", 2, 3, i) for i in PAIR],
}
F32 = jnp.float32
BF16 = jnp.bfloat16


def layer_kernel(
    n,
    n_tp,
    key_ref,
    val_ref,
    docs_ref,
    sink_ref,
    query_ref,
    out_proj_ref,
    residual_ref,
    mix_ref,
    gate_ref,
    value_ref,
    gate_taps_ref,
    value_taps_ref,
    down_ref,
    final_ref,
    out_ref,
    gate_all,
    value_all,
    down_all,
    key_ext,
    val_ext,
    docs_ext,
    docs_other,
    doc_cols,
    mask_cols,
    taps_gate,
    taps_value,
    queries,
    proj,
    rest,
    heads,
    parts,
    parts_in,
    norm_own,
    norm_cols,
    normed,
    up_gate,
    up_value,
    hidden,
    terms,
    terms_in,
    from_mate,
    second,
    stats,
    plane_send,
    onward_send,
    row_send,
    core_send,
    block_recv,
    core_recv,
    local_sem,
    taps_send,
    taps_recv,
    halo_send,
    halo_recv,
    rows_send,
    rows_recv,
    norm_send,
    norm_recv,
    pass_send,
    cols_send,
    cols_recv,
    tail_send,
    tail_recv,
    term_send,
    term_recv,
    mate_recv,
    stat_send,
    stat_recv,
):
    sp = lax.axis_index("sp")
    tp = lax.axis_index("tp")
    rows = query_ref.shape[0]
    ff = gate_ref.shape[1]
    width = residual_ref.shape[1]
    depth = gate_ref.shape[0]
    cols = down_ref.shape[1]
    share = width // n_tp
    per = share // cols
    planes = n // 2
    z, y = sp // 2, lax.rem(sp, 2)
    x, core = tp // 2, lax.rem(tp, 2)
    low = lax.rem(z, 2)
    half = z // 2
    inner = lax.rem(low + half, 2) == 1
    home = low == core
    base = sp - 2 * low
    work = base + 2 * core
    partner = base + 2 * (1 - low)
    sibling = 2 * x + 1 - core
    facing = 2 * (1 - x) + core
    across = 2 * z + 1 - y
    after = lax.rem(sp + 1, n)
    peers = [lax.rem(tp + i, n_tp) for i in range(1, n_tp)]
    everyone = n * n_tp
    me = sp * n_tp + tp
    row_share = rows // n_tp

    barrier = pltpu.get_barrier_semaphore()

    def greet(i, carry):
        other = lax.rem(me + i, everyone)
        pl.semaphore_signal(
            barrier,
            inc=1,
            device_id=(other // n_tp, lax.rem(other, n_tp)),
            device_id_type=MESH,
        )
        return carry

    lax.fori_loop(1, everyone, greet, 0)
    fetch = [
        pltpu.make_async_copy(key_ref, key_ext.at[:, pl.ds(WIN, rows)], local_sem.at[0]),
        pltpu.make_async_copy(val_ref, val_ext.at[:, pl.ds(WIN, rows)], local_sem.at[1]),
        pltpu.make_async_copy(docs_ref, docs_ext.at[:, pl.ds(WIN, rows)], local_sem.at[2]),
        pltpu.make_async_copy(query_ref, queries, local_sem.at[3]),
        pltpu.make_async_copy(out_proj_ref, proj, local_sem.at[4]),
        pltpu.make_async_copy(
            residual_ref.at[pl.ds(pl.multiple_of(tp * row_share, row_share), row_share)],
            rest,
            local_sem.at[5],
        ),
    ]
    for copy in fetch:
        copy.start()
    pl.semaphore_wait(barrier, everyone - 1)

    whole = (gate_all, value_all, down_all)
    own = (gate_ref, value_ref, down_ref)
    sizes = (depth // CHUNKS, depth // CHUNKS, ff // CHUNKS)

    def piece(w, q):
        return own[w].at[pl.ds(q * sizes[w], sizes[w])]

    def slot(w, index, q):
        if w == 2:
            return down_all.at[index, pl.ds(q * sizes[2], sizes[2])]
        return whole[w].at[
            pl.ds(pl.multiple_of(index * depth + q * sizes[w], sizes[w]), sizes[w])
        ]

    def slab(w, index):
        if w == 2:
            return down_all.at[index]
        return whole[w].at[pl.ds(pl.multiple_of(index * depth, depth), depth)]

    def to_plane(w, i, q):
        return pltpu.make_async_remote_copy(
            src_ref=piece(w, q),
            dst_ref=slot(w, sp, q),
            send_sem=plane_send.at[w, i, q],
            recv_sem=block_recv.at[w, sp, q],
            device_id=(2 * (core + 2 * i) + y, 2 * x + (core if q % 2 == 0 else 1 - core)),
            device_id_type=MESH,
        )

    def to_row(w, at, q, source, target):
        return pltpu.make_async_remote_copy(
            src_ref=source,
            dst_ref=slot(w, 2 * at + y, q),
            send_sem=row_send.at[w, at, q],
            recv_sem=block_recv.at[w, 2 * at + y, q],
            device_id=(across, target),
            device_id_type=MESH,
        )

    def to_core(w, index, q, source):
        return pltpu.make_async_remote_copy(
            src_ref=source,
            dst_ref=slot(w, index, q),
            send_sem=core_send.at[w, index, q],
            recv_sem=core_recv.at[w, index, q],
            device_id=(sp, sibling),
            device_id_type=MESH,
        )

    def await_piece(w, index, q):
        pltpu.make_async_remote_copy(
            src_ref=slot(w, index, q),
            dst_ref=slot(w, index, q),
            send_sem=core_send.at[w, index, q],
            recv_sem=block_recv.at[w, index, q],
            device_id=(sp, sibling),
            device_id_type=MESH,
        ).wait_recv()

    def near_sends(w):
        for i in range(2):
            @pl.when((half == i) & (core + 2 * i != z))
            def _():
                for q in range(CHUNKS):
                    to_plane(w, i, q).start()

    def far_sends(w, cond):
        for i in range(2):
            @pl.when((half != i) & cond)
            def _():
                for q in range(CHUNKS):
                    to_plane(w, i, q).start()

    def zone(k):
        block = lax.rem(half + k // 2, 2)
        side = low if k < 2 else half
        return 2 * block + lax.rem(side + k % 2, 2)

    def own_row(w):
        @pl.when(home)
        def _():
            for q in range(CHUNKS):
                to_row(w, z, q, piece(w, q), tp if q % 2 == 0 else sibling).start()

    def own_core(w):
        @pl.when(home)
        def _():
            for q in range(CHUNKS):
                to_core(w, sp, q, piece(w, q)).start()

    role = jnp.where(home, 0, 1)

    def onward(w, i):
        index, q = 2 * zone(1) + y, 2 * i + role
        return pltpu.make_async_remote_copy(
            src_ref=slot(w, index, q),
            dst_ref=slot(w, index, q),
            send_sem=onward_send.at[w, i],
            recv_sem=block_recv.at[w, index, q],
            device_id=(2 * (z + 2 - 4 * half) + y, tp),
            device_id_type=MESH,
        )

    def col(w, k, i):
        at, q = zone(k), 2 * i + role
        index = 2 * at + y
        await_piece(w, index, q)
        if k == 1:
            @pl.when(inner)
            def _():
                onward(w, i).start()

        to_row(w, at, q, slot(w, index, q), tp).start()
        to_core(w, index, q, slot(w, index, q)).start()

    def row(w, k, i):
        index, q = 2 * zone(k) + 1 - y, 2 * i + role
        await_piece(w, index, q)
        to_core(w, index, q, slot(w, index, q)).start()

    def serve(events):
        for kind, w, k, i in events:
            if kind == "far":
                far_sends(w, inner)
            elif kind == "norm":
                @pl.when(jnp.logical_not(home))
                def _():
                    for i in PAIR:
                        norm_copy(0, (sp, sibling), 2 * x + i).wait_recv()
                        norm_pass(i).start()

            else:
                (col if kind == "col" else row)(w, k, i)

    def await_slab(w, k, flip):
        index = 2 * zone(k) + (1 - y if flip else y)
        if k == 0 and not flip:
            @pl.when(jnp.logical_not(home))
            def _():
                for q in range(CHUNKS):
                    to_core(w, index, q, slot(w, index, q)).wait_recv()
        else:
            for i in range(CHUNKS // 2):
                q = 2 * i + 1 - role
                to_core(w, index, q, slot(w, index, q)).wait_recv()

    halo = [
        pltpu.make_async_remote_copy(
            src_ref=source,
            dst_ref=target,
            send_sem=halo_send.at[i],
            recv_sem=halo_recv.at[i],
            device_id=(after, tp),
            device_id_type=MESH,
        )
        for i, (source, target) in enumerate(
            (
                (ref.at[:, pl.ds(rows - WIN, WIN)], ext.at[:, pl.ds(0, WIN)])
                for ref, ext in (
                    (key_ref, key_ext),
                    (val_ref, val_ext),
                    (docs_ref, docs_ext),
                )
            )
        )
    ]
    for copy in halo:
        copy.start()
    near_sends(0)
    far_sends(0, inner | home)
    near_sends(1)
    near_sends(2)
    own_row(0)
    own_row(1)
    settle = [
        pltpu.make_async_copy(own[w], slab(w, sp), local_sem.at[6 + w]) for w in range(3)
    ]
    tap_pairs = ((gate_taps_ref, taps_gate), (value_taps_ref, taps_value))
    for i, (source, target) in enumerate(tap_pairs):
        settle.append(pltpu.make_async_copy(source, target, local_sem.at[9 + i]))
    taps = [
        pltpu.make_async_remote_copy(
            src_ref=source,
            dst_ref=target,
            send_sem=taps_send.at[i],
            recv_sem=taps_recv.at[i],
            device_id=(sp, sibling),
            device_id_type=MESH,
        )
        for i, (source, target) in enumerate(tap_pairs)
    ]

    @pl.when(home)
    def _():
        for copy in settle + taps:
            copy.start()

    own_core(0)
    own_core(1)
    own_core(2)
    for copy in fetch:
        copy.wait()

    line = lax.broadcasted_iota(jnp.int32, (LANES, LANES), 0)
    lane = lax.broadcasted_iota(jnp.int32, (LANES, LANES), 1)
    for b in range(1, rows // LANES + 1):
        row_doc = docs_ext[0:1, b * LANES : (b + 1) * LANES].astype(F32)
        doc_cols[b * LANES : (b + 1) * LANES, :] = jnp.broadcast_to(row_doc, (LANES, LANES)).T

    zero = jnp.zeros((HD, 2 * WIN), BF16)

    def pair_copy(i, block):
        return pltpu.make_async_remote_copy(
            src_ref=parts.at[block],
            dst_ref=parts_in.at[i],
            send_sem=rows_send.at[i],
            recv_sem=rows_recv.at[i],
            device_id=(sp, sibling),
            device_id_type=MESH,
        )

    def facing_copy():
        return pltpu.make_async_remote_copy(
            src_ref=parts.at[facing],
            dst_ref=parts_in.at[2],
            send_sem=rows_send.at[2],
            recv_sem=rows_recv.at[2],
            device_id=(sp, facing),
            device_id_type=MESH,
        )

    def attend_block(j, carry):
        b = 2 * lax.rem(x + 1 + j, 2) + lax.rem(core + 1 + j // 2, 2)

        @pl.when(b == 0)
        def _():
            for copy in halo:
                copy.wait_recv()

        start = pl.multiple_of(b * WIN, WIN)
        k = key_ext[:, pl.ds(start, 2 * WIN)]
        v = val_ext[:, pl.ds(start, 2 * WIN)]
        keys = jnp.concatenate(
            [jnp.concatenate([k, zero], axis=1), jnp.concatenate([zero, k], axis=1)], axis=0
        )
        values = jnp.concatenate(
            [jnp.concatenate([v, zero], axis=1), jnp.concatenate([zero, v], axis=1)], axis=0
        )
        query_doc = doc_cols[pl.ds(start + WIN, WIN), :]
        prev_doc = docs_ext[0:1, pl.ds(start, WIN)].astype(F32)
        this_doc = docs_ext[0:1, pl.ds(start + WIN, WIN)].astype(F32)
        prev_ok = (query_doc == prev_doc) & (lane > line) & (sp * rows + b * WIN > 0)
        this_ok = (query_doc == this_doc) & (lane <= line)
        bias = jnp.concatenate(
            [jnp.where(prev_ok, 0.0, -1e30), jnp.where(this_ok, 0.0, -1e30)], axis=1
        ).astype(F32)
        for pair in range(query_ref.shape[1] // LANES):
            block = queries[pl.ds(start, WIN), pair * LANES : (pair + 1) * LANES]
            both = jnp.dot(block, keys, preferred_element_type=F32)
            probs = []
            for side in (0, 1):
                scores = both[:, side * 2 * WIN : (side + 1) * 2 * WIN] * HD ** (-0.5) + bias
                sink = sink_ref[2 * pair + side]
                top = jnp.maximum(jnp.max(scores, axis=1, keepdims=True), sink)
                weights = jnp.exp(scores - top)
                total = jnp.sum(weights, axis=1, keepdims=True) + jnp.exp(sink - top)
                probs.append((weights / total).astype(BF16))
            heads[:, pair * LANES : (pair + 1) * LANES] = lax.dot_general(
                jnp.concatenate(probs, axis=1),
                values,
                (((1,), (1,)), ((), ())),
                preferred_element_type=F32,
            ).astype(BF16)
        for c in range(width // 512):
            parts[b, :, c * 512 : (c + 1) * 512] = jnp.dot(
                heads[...], proj[:, c * 512 : (c + 1) * 512], preferred_element_type=F32
            ).astype(BF16)

        @pl.when(j == 0)
        def _():
            pair_copy(0, 2 * (1 - x) + 1 - core).start()

        @pl.when(j == 1)
        def _():
            pair_copy(1, sibling).start()

        @pl.when(j == 2)
        def _():
            pair_copy(0, facing).wait_recv()
            parts[facing] = (parts[facing].astype(F32) + parts_in[0].astype(F32)).astype(BF16)
            facing_copy().start()

        return carry

    lax.fori_loop(0, n_tp, attend_block, 0)

    serve(EARLY)
    own_row(2)
    pair_copy(1, tp).wait_recv()
    facing_copy().wait_recv()
    first = mix_scale * rest[...].astype(F32) + parts[tp].astype(F32)
    first = first + parts_in[1].astype(F32) + parts_in[2].astype(F32)
    mean = jnp.mean(first, axis=1, keepdims=True)
    first = first - mean
    var = jnp.mean(first * first, axis=1, keepdims=True)
    norm_own[...] = (first * lax.rsqrt(var + norm_eps) * mix_ref[...]).astype(BF16)

    def workers(block):
        parity = lax.rem(block // 2, 2)
        return [
            (block - 2 * parity + 2 * a, 2 * b + parity)
            for a in (0, 1)
            for b in range(n_tp // 2)
        ]

    def place_of(source):
        return pl.ds(pl.multiple_of(PAD + source * row_share, PAD), row_share)

    def norm_copy(i, device, source):
        return pltpu.make_async_remote_copy(
            src_ref=norm_own,
            dst_ref=normed.at[place_of(source)],
            send_sem=norm_send.at[i],
            recv_sem=norm_recv.at[source],
            device_id=device,
            device_id_type=MESH,
        )

    def takes(i, device):
        return jnp.where(device[0] == sp, device[1] != tp, x == i % 2)

    def norm_pass(i):
        return pltpu.make_async_remote_copy(
            src_ref=normed.at[place_of(2 * x + i)],
            dst_ref=normed.at[place_of(2 * x + i)],
            send_sem=pass_send.at[i],
            recv_sem=norm_recv.at[2 * x + i],
            device_id=(sp, facing),
            device_id_type=MESH,
        )

    def cols_copy(i, peer, source):
        rows_at = pl.ds(pl.multiple_of(source * row_share, row_share), row_share)
        return pltpu.make_async_remote_copy(
            src_ref=norm_own.at[:, pl.ds(pl.multiple_of(peer * share, share), share)],
            dst_ref=norm_cols.at[rows_at],
            send_sem=cols_send.at[i],
            recv_sem=cols_recv.at[source],
            device_id=(sp, peer),
            device_id_type=MESH,
        )

    def tail_copy(i, device):
        return pltpu.make_async_remote_copy(
            src_ref=norm_own.at[pl.ds(row_share - PAD // 2, PAD // 2)],
            dst_ref=normed.at[pl.ds(PAD // 2, PAD // 2)],
            send_sem=tail_send.at[i],
            recv_sem=tail_recv,
            device_id=device,
            device_id_type=MESH,
        )

    own_workers = workers(sp)
    next_workers = workers(after)

    @pl.when((tp == n_tp - 1) & (sp < n - 1))
    def _():
        for i, device in enumerate(next_workers):
            tail_copy(i, device).start()

    for i, device in enumerate(own_workers):
        @pl.when(takes(i, device))
        def _():
            norm_copy(i, device, tp).start()

    far_sends(1, home & jnp.logical_not(inner))
    far_sends(2, home & jnp.logical_not(inner))
    for i, peer in enumerate(peers):
        cols_copy(i, peer, tp).start()

    docs_copy = pltpu.make_async_remote_copy(
        src_ref=docs_ext,
        dst_ref=docs_other,
        send_sem=halo_send.at[3],
        recv_sem=halo_recv.at[3],
        device_id=(partner, tp),
        device_id_type=MESH,
    )
    docs_copy.start()

    @pl.when(home)
    def _():
        normed[place_of(tp), :] = norm_own[...]

    norm_cols[pl.ds(pl.multiple_of(tp * row_share, row_share), row_share), :] = norm_own[
        :, pl.ds(pl.multiple_of(tp * share, share), share)
    ]

    serve(MIDDLE)
    docs_copy.wait_recv()
    place = lax.broadcasted_iota(jnp.int32, (LANES, LANES), 0)
    for b in range(rows // LANES):
        now = slice(WIN + b * LANES, WIN + (b + 1) * LANES)
        before = slice(b * LANES, (b + 1) * LANES)
        doc_now = jnp.where(home, docs_ext[0:1, now], docs_other[0:1, now]).astype(F32)
        doc_before = jnp.where(home, docs_ext[0:1, before], docs_other[0:1, before]).astype(F32)
        tall = jnp.broadcast_to(doc_now, (LANES, LANES)).T
        ahead = jnp.broadcast_to(doc_before, (LANES, LANES)).T
        mask_cols[0, PAD + b * LANES : PAD + (b + 1) * LANES, :] = tall
        if b == 0:
            mask_cols[0, 0:PAD, :] = ahead[LANES - PAD :]
    for b in range(rows // LANES):
        at = PAD + b * LANES
        doc = mask_cols[0, at : at + LANES, :]
        for lag in range(1, TAPS):
            same = (mask_cols[0, at - lag : at - lag + LANES, :] == doc) & (
                place + (work * rows + b * LANES) >= lag
            )
            mask_cols[lag, at : at + LANES, :] = jnp.where(same, 1.0, 0.0).astype(F32)

    for source in range(n_tp):
        @pl.when(jnp.where(home, tp != source, x != source // 2))
        def _():
            norm_copy(0, (sp, sibling), source).wait_recv()

    @pl.when(work > 0)
    def _():
        tail_copy(0, (sp, sibling)).wait_recv()

    @pl.when(work == 0)
    def _():
        normed[0:PAD, :] = jnp.zeros((PAD, width), BF16)


    @pl.when(home)
    def _():
        for copy in settle:
            copy.wait()

    @pl.when(jnp.logical_not(home))
    def _():
        for copy in taps:
            copy.wait_recv()

    for w in (0, 1):
        for k in range(planes):
            for flip in (0, 1):
                await_slab(w, k, flip)

    def convolved(source, taps_ref, at):
        total = taps_ref[0:1, pl.ds(at, LANES)] * source[PAD : PAD + rows, :]
        for lag in range(1, TAPS):
            tap = taps_ref[lag : lag + 1, pl.ds(at, LANES)]
            shifted = source[PAD - lag : PAD - lag + rows, :]
            total = total + tap * (shifted * mask_cols[lag, PAD : PAD + rows, :])
        return total

    def project(c, pair):
        at = pl.multiple_of(c * LANES, LANES)
        weights = jnp.concatenate(
            [gate_all[:, pl.ds(at, LANES)], value_all[:, pl.ds(at, LANES)]], axis=1
        )
        both = jnp.dot(normed[...], weights, preferred_element_type=F32)
        both = both.astype(BF16).astype(F32)
        pair[0][...] = both[:, :LANES]
        pair[1][...] = both[:, LANES:]

    def activate(c, pair):
        at = pl.multiple_of(c * LANES, LANES)
        gate = convolved(pair[0], taps_gate, at)
        value = convolved(pair[1], taps_value, at)
        inside = math.sqrt(2.0 / math.pi) * (gate + 0.044715 * (gate * gate * gate))
        hidden[:, pl.ds(at, LANES)] = (0.5 * gate * (1.0 + jnp.tanh(inside)) * value).astype(BF16)

    even, odd = (up_gate.at[0], up_value.at[0]), (up_gate.at[1], up_value.at[1])
    steps = ff // LANES
    project(0, even)

    def up_block(d, carry):
        c = 2 * d
        activate(c, even)
        project(c + 1, odd)
        activate(c + 1, odd)
        project(c + 2, even)
        for at_step, events in UP_SERVE:
            @pl.when(d == at_step)
            def _():
                serve(events)

        return carry

    lax.fori_loop(0, (steps - 1) // 2, up_block, 0)
    activate(steps - 1, even)

    def term_copy(index, target, where, sem, device):
        return pltpu.make_async_remote_copy(
            src_ref=terms.at[index],
            dst_ref=target.at[where],
            send_sem=term_send.at[index],
            recv_sem=sem.at[where],
            device_id=device,
            device_id_type=MESH,
        )

    def to_owner(index, source, device):
        return term_copy(index, terms_in, per * source + lax.rem(index, per), term_recv, device)

    def to_mate(index, over_x):
        device = (sp, facing) if over_x else (work, tp)
        return term_copy(index, from_mate, lax.rem(index, 2 * per), mate_recv, device)

    def slab_index(k, flip):
        return 2 * zone(k) + (1 - y if flip else y)

    def down_block(k, flip):
        index = slab_index(k, flip)
        owner = index // per
        crossing = owner // 2 != x
        serve(DOWN_SERVE.get((k, flip), ()))
        await_slab(2, k, flip)
        terms[index] = jnp.dot(
            hidden[...], down_all[index], preferred_element_type=F32
        ).astype(BF16)

        @pl.when(home & (owner == tp))
        def _():
            terms_in[lax.rem(index, per)] = terms[index]

        @pl.when(home & (owner == sibling))
        def _():
            to_owner(index, 0, (sp, sibling)).start()

        if (k, flip) in X_FIRST:
            @pl.when(home & crossing)
            def _():
                to_owner(index, 2, (sp, owner)).start()
        else:
            @pl.when(jnp.logical_not(home | crossing))
            def _():
                to_owner(index, 1, (work, owner)).start()

        @pl.when(jnp.logical_not(home) & crossing)
        def _():
            to_mate(index, (k, flip) in X_FIRST).start()

    def cross_block(k, flip):
        index = slab_index(k, flip)
        owner = index // per

        crossing = owner // 2 != x

        over_x = (k, flip) in X_FIRST

        @pl.when(jnp.logical_not(home | crossing) if over_x else home & crossing)
        def _():
            to_mate(index, over_x).wait_recv()
            terms[index] = (
                terms[index].astype(F32) + from_mate[lax.rem(index, 2 * per)].astype(F32)
            ).astype(BF16)
            if over_x:
                to_owner(index, 1, (work, owner)).start()
            else:
                to_owner(index, 2, (sp, owner)).start()

    for step, k, flip in DOWN_ORDER:
        (down_block if step == "down" else cross_block)(k, flip)

    for source in range(3):
        @pl.when(jnp.logical_not(home) if source == 0 else tp >= 0)
        def _():
            for j in range(per):
                term_copy(
                    0, terms_in, per * source + j, term_recv, (sp, sibling)
                ).wait_recv()

    for i, peer in enumerate(peers):
        cols_copy(i, peer, peer).wait_recv()

    sums = jnp.zeros((rows, 1), F32)
    squares = jnp.zeros((rows, 1), F32)
    for j in range(per):
        total = mix_scale * norm_cols[:, j * cols : (j + 1) * cols].astype(F32)
        for source in range(3):
            total = total + terms_in[per * source + j].astype(F32)
        second[:, j * cols : (j + 1) * cols] = total
        sums = sums + jnp.sum(total, axis=1, keepdims=True)
        squares = squares + jnp.sum(total * total, axis=1, keepdims=True)
    which = lax.broadcasted_iota(jnp.int32, (rows, LANES), 1)
    packed = jnp.where(which == 0, sums, jnp.where(which == 1, squares, 0.0))
    stats[tp] = packed.T[0:8]

    def stat_copy(peer, source):
        return pltpu.make_async_remote_copy(
            src_ref=stats.at[source],
            dst_ref=stats.at[source],
            send_sem=stat_send.at[peer],
            recv_sem=stat_recv.at[source],
            device_id=(sp, peer),
            device_id_type=MESH,
        )

    for peer in peers:
        stat_copy(peer, tp).start()

    for w in range(3):
        for i in range(2):
            @pl.when((core + 2 * i != z) & ((half == i) | inner | home))
            def _():
                for q in range(CHUNKS):
                    to_plane(w, i, q).wait_send()

        @pl.when(inner)
        def _():
            for i in range(CHUNKS // 2):
                onward(w, i).wait_send()

    for k in range(planes):
        at = zone(k)
        for w in range(3):
            for i in range(CHUNKS // 2):
                q = 2 * i + role
                if k > 0:
                    index = 2 * at + y
                    to_row(w, at, q, slot(w, index, q), tp).wait_send()
                    to_core(w, index, q, slot(w, index, q)).wait_send()
                index = 2 * at + 1 - y
                to_core(w, index, q, slot(w, index, q)).wait_send()

    @pl.when(home)
    def _():
        for w in range(3):
            for q in range(CHUNKS):
                to_row(w, z, q, piece(w, q), tp if q % 2 == 0 else sibling).wait_send()
                to_core(w, sp, q, piece(w, q)).wait_send()
        for copy in taps:
            copy.wait_send()

    for copy in halo:
        copy.wait_send()
    docs_copy.wait_send()
    for i, device in enumerate(own_workers):
        @pl.when(takes(i, device))
        def _():
            norm_copy(i, device, tp).wait_send()

    @pl.when(jnp.logical_not(home))
    def _():
        for i in PAIR:
            norm_pass(i).wait_send()

    @pl.when((tp == n_tp - 1) & (sp < n - 1))
    def _():
        for i, device in enumerate(next_workers):
            tail_copy(i, device).wait_send()

    pair_copy(0, 2 * (1 - x) + 1 - core).wait_send()
    pair_copy(1, sibling).wait_send()
    facing_copy().wait_send()
    for i, peer in enumerate(peers):
        cols_copy(i, peer, tp).wait_send()
    for index in range(n):
        @pl.when(jnp.logical_not(home & (tp == index // per)))
        def _():
            to_mate(index, 0).wait_send()

    for peer in peers:
        stat_copy(peer, peer).wait_recv()
    total = stats[0]
    for source in range(1, n_tp):
        total = total + stats[source]
    spread = jnp.concatenate([total] * (LANES // 8), axis=0).T
    mean = spread[:, 0:1] / width
    var = spread[:, 1:2] / width - mean * mean
    out_ref[...] = (
        (second[...] - mean) * lax.rsqrt(var + norm_eps) * final_ref[...]
    ).astype(BF16)
    for peer in peers:
        stat_copy(peer, tp).wait_send()


def fused(
    query_rows,
    key_rows,
    value_rows,
    doc_ids,
    sink_logit,
    residual,
    out_proj,
    mix_gain,
    gate_proj,
    value_proj,
    gate_taps,
    value_taps,
    down_proj,
    final_gain,
):
    n = lax.axis_size("sp")
    n_tp = lax.axis_size("tp")
    rows, head_cols = query_rows.shape
    width = residual.shape[1]
    depth, ff = gate_proj.shape
    cols = down_proj.shape[1]
    per = width // n_tp // cols
    planes = n // 2
    share = rows // n_tp
    anywhere = pl.BlockSpec(memory_space=pl.ANY)
    vmem = pl.BlockSpec(memory_space=pltpu.VMEM)
    smem = pl.BlockSpec(memory_space=pltpu.SMEM)
    dma = pltpu.SemaphoreType.DMA
    return pl.pallas_call(
        functools.partial(layer_kernel, n, n_tp),
        out_shape=jax.ShapeDtypeStruct((rows, width // n_tp), BF16),
        in_specs=[
            anywhere, anywhere, anywhere, smem, anywhere, anywhere, anywhere, vmem,
            anywhere, anywhere, anywhere, anywhere, anywhere, vmem,
        ],
        out_specs=vmem,
        scratch_shapes=[
            pltpu.VMEM((n * depth, ff), BF16),
            pltpu.VMEM((n * depth, ff), BF16),
            pltpu.VMEM((n, ff, cols), BF16),
            pltpu.VMEM((HD, WIN + rows), BF16),
            pltpu.VMEM((HD, WIN + rows), BF16),
            pltpu.VMEM((1, WIN + rows), jnp.int32),
            pltpu.VMEM((1, WIN + rows), jnp.int32),
            pltpu.VMEM((WIN + rows, LANES), F32),
            pltpu.VMEM((TAPS, PAD + rows, LANES), F32),
            pltpu.VMEM(gate_taps.shape, F32),
            pltpu.VMEM(value_taps.shape, F32),
            pltpu.VMEM((rows, head_cols), BF16),
            pltpu.VMEM((head_cols, width), BF16),
            pltpu.VMEM((share, width), BF16),
            pltpu.VMEM((share, head_cols), BF16),
            pltpu.VMEM((n_tp, share, width), BF16),
            pltpu.VMEM((3, share, width), BF16),
            pltpu.VMEM((share, width), BF16),
            pltpu.VMEM((rows, width // n_tp), BF16),
            pltpu.VMEM((PAD + rows, width), BF16),
            pltpu.VMEM((2, PAD + rows, LANES), F32),
            pltpu.VMEM((2, PAD + rows, LANES), F32),
            pltpu.VMEM((rows, ff), BF16),
            pltpu.VMEM((n, rows, cols), BF16),
            pltpu.VMEM((3 * per, rows, cols), BF16),
            pltpu.VMEM((2 * per, rows, cols), BF16),
            pltpu.VMEM((rows, width // n_tp), F32),
            pltpu.VMEM((n_tp, 8, rows), F32),
            dma((3, 2, CHUNKS)),
            dma((3, CHUNKS // 2)),
            dma((3, planes, CHUNKS)),
            dma((3, n, CHUNKS)),
            dma((3, n, CHUNKS)),
            dma((3, n, CHUNKS)),
            dma((11,)),
            dma((2,)),
            dma((2,)),
            dma((4,)),
            dma((4,)),
            dma((3,)),
            dma((3,)),
            dma((n_tp,)),
            dma((n_tp,)),
            dma((2,)),
            dma((n_tp,)),
            dma((n_tp,)),
            dma((n_tp,)),
            dma(()),
            dma((n,)),
            dma((3 * per,)),
            dma((2 * per,)),
            dma((n_tp,)),
            dma((n_tp,)),
        ],
        compiler_params=pltpu.CompilerParams(
            collective_id=0, has_side_effects=True, vmem_limit_bytes=60 * 1024 * 1024
        ),
        name="layer",
    )(
        key_rows.T,
        value_rows.T,
        doc_ids[None, :],
        sink_logit,
        query_rows,
        out_proj,
        residual,
        mix_gain[None, :],
        gate_proj,
        value_proj,
        gate_taps,
        value_taps,
        down_proj,
        final_gain[None, :],
    )


def on_any(*args):
    query_rows, key_rows, gate_proj, down_proj = args[0], args[1], args[8], args[12]
    n, n_tp = lax.axis_size("sp"), lax.axis_size("tp")
    share = args[5].shape[1] // n_tp
    depth, ff = gate_proj.shape
    cols = down_proj.shape[1]
    fits = (
        n == 8
        and n_tp == 4
        and ff >= 10 * LANES
        and query_rows.shape[0] == n_tp * WIN
        and key_rows.shape[1] == HD
        and query_rows.shape[1] % LANES == 0
        and depth % (16 * CHUNKS) == 0
        and ff % (2 * LANES) == LANES
        and ff % (16 * CHUNKS) == 0
        and cols % LANES == 0
        and share % cols == 0
    )
    return fused(*args) if fits else on_device(*args)


def solution(mesh):
    placed = (
        P("sp", "tp"),
        P("sp", "tp"),
        P("sp", "tp"),
        P("sp"),
        P("tp"),
        P("sp", None),
        P("tp", None),
        P(),
        P("sp", "tp"),
        P("sp", "tp"),
        P(None, "tp"),
        P(None, "tp"),
        P("tp", "sp"),
        P("tp"),
    )
    return jax.shard_map(
        on_any, mesh=mesh, in_specs=placed, out_specs=P("sp", "tp"), check_vma=False
    )
```

```python
import functools
import math

import jax
import jax.numpy as jnp
from jax import lax
from jax.experimental import pallas as pl
from jax.experimental.pallas import tpu as pltpu
from jax.sharding import PartitionSpec as P

HD = 64
WIN = 128
TAPS = 3


mix_scale = math.sqrt(2.0)
norm_eps = 1e-05


def passed_along(block, axis, distance):
    devices = range(lax.axis_size(axis))
    route = [(i - distance, i) for i in devices if i - distance in devices]
    return lax.ppermute(block, axis, route)


def attend(query_block, key_block, value_block, query_pos, key_pos, query_doc, key_doc, sink):
    head_size = query_block.shape[-1]
    scores = jnp.einsum(
        "qkgd,skd->kgqs", query_block, key_block, preferred_element_type=jnp.float32
    ) * head_size ** (-0.5)
    diff = query_pos[:, None] - key_pos[None, :]
    valid = (
        (diff >= 0)
        & (diff < WIN)
        & (query_doc[:, None] == key_doc[None, :])
        & (key_pos[None, :] >= 0)
    )
    scores = jnp.where(valid[None, None], scores, -1e30)
    top = jnp.maximum(jnp.max(scores, axis=-1, keepdims=True), sink)
    weights = jnp.exp(scores - top)
    total = jnp.sum(weights, axis=-1, keepdims=True) + jnp.exp(sink - top)
    probs = (weights / total).astype(jnp.bfloat16)
    out = jnp.einsum("kgqs,skd->qkgd", probs, value_block, preferred_element_type=jnp.float32)
    return out.astype(jnp.bfloat16)


def depthwise(tail, current, taps, tail_docs, docs):
    extended = jnp.concatenate([tail, current])
    ext_docs = jnp.concatenate([tail_docs, docs])
    lag_rows = tail.shape[0]
    count = current.shape[0]
    total = jnp.zeros(current.shape, jnp.float32)
    for lag in range(lag_rows + 1):
        start = lag_rows - lag
        same = (ext_docs[start : start + count] == docs)[:, None]
        rows = extended[start : start + count].astype(jnp.float32)
        total = total + taps[lag][None, :] * jnp.where(same, rows, 0.0)
    return total


def on_device(
    query_rows,
    key_rows,
    value_rows,
    doc_ids,
    sink_logit,
    residual,
    out_proj,
    mix_gain,
    gate_proj,
    value_proj,
    gate_taps,
    value_taps,
    down_proj,
    final_gain,
):
    rows = query_rows.shape[0]
    kv_local = key_rows.shape[1] // HD
    heads_local = query_rows.shape[1] // HD
    groups = heads_local // kv_local
    offset = lax.axis_index("sp") * rows
    prev_keys, prev_values, prev_docs = passed_along(
        (key_rows[rows - WIN :], value_rows[rows - WIN :], doc_ids[rows - WIN :]), "sp", 1
    )
    all_keys = jnp.concatenate([prev_keys, key_rows]).reshape(rows + WIN, kv_local, HD)
    all_values = jnp.concatenate([prev_values, value_rows]).reshape(rows + WIN, kv_local, HD)
    all_docs = jnp.concatenate([prev_docs, doc_ids])
    key_pos = offset - WIN + jnp.arange(rows + WIN, dtype=jnp.int32)
    query_pos = offset + jnp.arange(rows, dtype=jnp.int32)
    queries = query_rows.reshape(rows, kv_local, groups, HD)
    sink = sink_logit.reshape(kv_local, groups, 1, 1)
    pieces = attend(queries, all_keys, all_values, query_pos, key_pos, doc_ids, all_docs, sink)
    heads = pieces.reshape(rows, heads_local * HD)
    partial_value = jnp.dot(heads, out_proj, preferred_element_type=jnp.float32)
    width = residual.shape[1]
    share = width // lax.axis_size("tp")
    col_start = lax.axis_index("tp") * share
    attn_total = lax.psum(partial_value.astype(jnp.bfloat16), "tp").astype(jnp.float32)
    first_sum = mix_scale * residual.astype(jnp.float32) + attn_total
    mean = jnp.mean(first_sum, axis=1, keepdims=True)
    var = jnp.mean(jnp.square(first_sum - mean), axis=1, keepdims=True)
    normed = ((first_sum - mean) * lax.rsqrt(var + norm_eps) * mix_gain[None, :]).astype(
        jnp.bfloat16
    )
    normed_own = lax.dynamic_slice_in_dim(normed, col_start, share, 1)
    up_gate = jnp.dot(
        normed,
        lax.all_gather(gate_proj, "sp", axis=0, tiled=True),
        preferred_element_type=jnp.float32,
    )
    up_value = jnp.dot(
        normed,
        lax.all_gather(value_proj, "sp", axis=0, tiled=True),
        preferred_element_type=jnp.float32,
    )
    up_gate = up_gate.astype(jnp.bfloat16)
    up_value = up_value.astype(jnp.bfloat16)
    lag_rows = TAPS - 1
    prev_gate, prev_value = passed_along(
        (up_gate[rows - lag_rows :], up_value[rows - lag_rows :]), "sp", 1
    )
    tail_docs = prev_docs[WIN - lag_rows :]
    conv_gate = depthwise(prev_gate, up_gate, gate_taps, tail_docs, doc_ids)
    conv_value = depthwise(prev_value, up_value, value_taps, tail_docs, doc_ids)
    hidden = (jax.nn.gelu(conv_gate) * conv_value).astype(jnp.bfloat16)
    terms = jnp.dot(
        hidden,
        lax.all_gather(down_proj, "sp", axis=1, tiled=True),
        preferred_element_type=jnp.float32,
    )
    ffn_own = lax.psum_scatter(
        terms.astype(jnp.bfloat16), "tp", scatter_dimension=1, tiled=True
    ).astype(jnp.float32)
    second_sum = mix_scale * normed_own.astype(jnp.float32) + ffn_own
    row_sum, row_squares = lax.psum(
        (jnp.sum(second_sum, axis=1), jnp.sum(second_sum * second_sum, axis=1)), "tp"
    )
    mean = row_sum / width
    var = row_squares / width - mean * mean
    return (
        (second_sum - mean[:, None]) * lax.rsqrt(var + norm_eps)[:, None] * final_gain[None, :]
    ).astype(jnp.bfloat16)


MESH = pl.DeviceIdType.MESH
LANES = 128
PAD = 16
CHUNKS = 4
PAIR = (0, 1)
EARLY = (
    [("col", 0, 1, i) for i in PAIR]
    + [("far", 1, 0, 0)]
    + [("row", 0, 0, i) for i in PAIR]
    + [("row", 1, 0, i) for i in PAIR]
)
MIDDLE = (
    [("col", 1, 1, i) for i in PAIR]
    + [("far", 2, 0, 0)]
    + [(kind, 0, k, i) for i in PAIR for kind, k in (("col", 2), ("col", 3), ("row", 1))]
    + [("norm", 0, 0, 0)]
    + [("row", 1, 1, i) for i in PAIR]
    + [(kind, w, k, i) for i in PAIR for w, kind, k in ((1, "col", 2), (0, "row", 2), (1, "col", 3), (0, "row", 3))]
    + [("col", 2, 1, i) for i in PAIR]
    + [("row", 1, k, i) for i in PAIR for k in (2, 3)]
)
UP_SERVE = (
    (0, [("row", 2, 0, i) for i in PAIR]),
    (1, [("row", 2, 1, i) for i in PAIR]),
    (2, [("col", 2, 2, 0)]),
    (3, [("col", 2, 2, 1), ("col", 2, 3, 0)]),
    (4, [("col", 2, 3, 1)]),
)
X_FIRST = ((0, 1), (1, 1))
DOWN_ORDER = (
    ("down", 0, 0),
    ("down", 0, 1),
    ("down", 1, 0),
    ("down", 1, 1),
    ("down", 2, 0),
    ("down", 3, 0),
    ("down", 2, 1),
    ("cross", 2, 0),
    ("down", 3, 1),
    ("cross", 0, 0),
    ("cross", 0, 1),
    ("cross", 1, 0),
    ("cross", 1, 1),
    ("cross", 3, 0),
    ("cross", 2, 1),
    ("cross", 3, 1),
)
DOWN_SERVE = {
    (2, 1): [("row", 2, 2, i) for i in PAIR],
    (3, 1): [("row", 2, 3, i) for i in PAIR],
}
F32 = jnp.float32
BF16 = jnp.bfloat16


def layer_kernel(
    n,
    n_tp,
    key_ref,
    val_ref,
    docs_ref,
    sink_ref,
    query_ref,
    out_proj_ref,
    residual_ref,
    mix_ref,
    gate_ref,
    value_ref,
    gate_taps_ref,
    value_taps_ref,
    down_ref,
    final_ref,
    out_ref,
    gate_all,
    value_all,
    down_all,
    key_ext,
    val_ext,
    docs_ext,
    docs_other,
    doc_cols,
    mask_cols,
    taps_gate,
    taps_value,
    queries,
    proj,
    rest,
    heads,
    parts,
    parts_in,
    norm_own,
    norm_cols,
    normed,
    up_gate,
    up_value,
    hidden,
    terms,
    terms_in,
    from_mate,
    second,
    stats,
    plane_send,
    onward_send,
    row_send,
    core_send,
    block_recv,
    core_recv,
    local_sem,
    taps_send,
    taps_recv,
    halo_send,
    halo_recv,
    rows_send,
    rows_recv,
    norm_send,
    norm_recv,
    pass_send,
    cols_send,
    cols_recv,
    tail_send,
    tail_recv,
    term_send,
    term_recv,
    mate_recv,
    stat_send,
    stat_recv,
):
    sp = lax.axis_index("sp")
    tp = lax.axis_index("tp")
    rows = query_ref.shape[0]
    ff = gate_ref.shape[1]
    width = residual_ref.shape[1]
    depth = gate_ref.shape[0]
    cols = down_ref.shape[1]
    share = width // n_tp
    per = share // cols
    planes = n // 2
    z, y = sp // 2, lax.rem(sp, 2)
    x, core = tp // 2, lax.rem(tp, 2)
    low = lax.rem(z, 2)
    half = z // 2
    inner = lax.rem(low + half, 2) == 1
    home = low == core
    base = sp - 2 * low
    work = base + 2 * core
    partner = base + 2 * (1 - low)
    sibling = 2 * x + 1 - core
    facing = 2 * (1 - x) + core
    across = 2 * z + 1 - y
    after = lax.rem(sp + 1, n)
    peers = [lax.rem(tp + i, n_tp) for i in range(1, n_tp)]
    everyone = n * n_tp
    me = sp * n_tp + tp
    row_share = rows // n_tp

    barrier = pltpu.get_barrier_semaphore()

    def greet(i, carry):
        other = lax.rem(me + i, everyone)
        pl.semaphore_signal(
            barrier,
            inc=1,
            device_id=(other // n_tp, lax.rem(other, n_tp)),
            device_id_type=MESH,
        )
        return carry

    lax.fori_loop(1, everyone, greet, 0)
    fetch = [
        pltpu.make_async_copy(key_ref, key_ext.at[:, pl.ds(WIN, rows)], local_sem.at[0]),
        pltpu.make_async_copy(val_ref, val_ext.at[:, pl.ds(WIN, rows)], local_sem.at[1]),
        pltpu.make_async_copy(docs_ref, docs_ext.at[:, pl.ds(WIN, rows)], local_sem.at[2]),
        pltpu.make_async_copy(query_ref, queries, local_sem.at[3]),
        pltpu.make_async_copy(out_proj_ref, proj, local_sem.at[4]),
        pltpu.make_async_copy(
            residual_ref.at[pl.ds(pl.multiple_of(tp * row_share, row_share), row_share)],
            rest,
            local_sem.at[5],
        ),
    ]
    for copy in fetch:
        copy.start()
    pl.semaphore_wait(barrier, everyone - 1)

    whole = (gate_all, value_all, down_all)
    own = (gate_ref, value_ref, down_ref)
    sizes = (depth // CHUNKS, depth // CHUNKS, ff // CHUNKS)

    def piece(w, q):
        return own[w].at[pl.ds(q * sizes[w], sizes[w])]

    def slot(w, index, q):
        if w == 2:
            return down_all.at[index, pl.ds(q * sizes[2], sizes[2])]
        return whole[w].at[
            pl.ds(pl.multiple_of(index * depth + q * sizes[w], sizes[w]), sizes[w])
        ]

    def slab(w, index):
        if w == 2:
            return down_all.at[index]
        return whole[w].at[pl.ds(pl.multiple_of(index * depth, depth), depth)]

    def to_plane(w, i, q):
        return pltpu.make_async_remote_copy(
            src_ref=piece(w, q),
            dst_ref=slot(w, sp, q),
            send_sem=plane_send.at[w, i, q],
            recv_sem=block_recv.at[w, sp, q],
            device_id=(2 * (core + 2 * i) + y, 2 * x + (core if q % 2 == 0 else 1 - core)),
            device_id_type=MESH,
        )

    def to_row(w, at, q, source, target):
        return pltpu.make_async_remote_copy(
            src_ref=source,
            dst_ref=slot(w, 2 * at + y, q),
            send_sem=row_send.at[w, at, q],
            recv_sem=block_recv.at[w, 2 * at + y, q],
            device_id=(across, target),
            device_id_type=MESH,
        )

    def to_core(w, index, q, source):
        return pltpu.make_async_remote_copy(
            src_ref=source,
            dst_ref=slot(w, index, q),
            send_sem=core_send.at[w, index, q],
            recv_sem=core_recv.at[w, index, q],
            device_id=(sp, sibling),
            device_id_type=MESH,
        )

    def await_piece(w, index, q):
        pltpu.make_async_remote_copy(
            src_ref=slot(w, index, q),
            dst_ref=slot(w, index, q),
            send_sem=core_send.at[w, index, q],
            recv_sem=block_recv.at[w, index, q],
            device_id=(sp, sibling),
            device_id_type=MESH,
        ).wait_recv()

    def near_sends(w):
        for i in range(2):
            @pl.when((half == i) & (core + 2 * i != z))
            def _():
                for q in range(CHUNKS):
                    to_plane(w, i, q).start()

    def far_sends(w, cond):
        for i in range(2):
            @pl.when((half != i) & cond)
            def _():
                for q in range(CHUNKS):
                    to_plane(w, i, q).start()

    def zone(k):
        block = lax.rem(half + k // 2, 2)
        side = low if k < 2 else half
        return 2 * block + lax.rem(side + k % 2, 2)

    def own_row(w):
        @pl.when(home)
        def _():
            for q in range(CHUNKS):
                to_row(w, z, q, piece(w, q), tp if q % 2 == 0 else sibling).start()

    def own_core(w):
        @pl.when(home)
        def _():
            for q in range(CHUNKS):
                to_core(w, sp, q, piece(w, q)).start()

    role = jnp.where(home, 0, 1)

    def onward(w, i):
        index, q = 2 * zone(1) + y, 2 * i + role
        return pltpu.make_async_remote_copy(
            src_ref=slot(w, index, q),
            dst_ref=slot(w, index, q),
            send_sem=onward_send.at[w, i],
            recv_sem=block_recv.at[w, index, q],
            device_id=(2 * (z + 2 - 4 * half) + y, tp),
            device_id_type=MESH,
        )

    def col(w, k, i):
        at, q = zone(k), 2 * i + role
        index = 2 * at + y
        await_piece(w, index, q)
        if k == 1:
            @pl.when(inner)
            def _():
                onward(w, i).start()

        to_row(w, at, q, slot(w, index, q), tp).start()
        to_core(w, index, q, slot(w, index, q)).start()

    def row(w, k, i):
        index, q = 2 * zone(k) + 1 - y, 2 * i + role
        await_piece(w, index, q)
        to_core(w, index, q, slot(w, index, q)).start()

    def serve(events):
        for kind, w, k, i in events:
            if kind == "far":
                far_sends(w, inner)
            elif kind == "norm":
                @pl.when(jnp.logical_not(home))
                def _():
                    for i in PAIR:
                        norm_copy(0, (sp, sibling), 2 * x + i).wait_recv()
                        norm_pass(i).start()

            else:
                (col if kind == "col" else row)(w, k, i)

    def await_slab(w, k, flip):
        index = 2 * zone(k) + (1 - y if flip else y)
        if k == 0 and not flip:
            @pl.when(jnp.logical_not(home))
            def _():
                for q in range(CHUNKS):
                    to_core(w, index, q, slot(w, index, q)).wait_recv()
        else:
            for i in range(CHUNKS // 2):
                q = 2 * i + 1 - role
                to_core(w, index, q, slot(w, index, q)).wait_recv()

    halo = [
        pltpu.make_async_remote_copy(
            src_ref=source,
            dst_ref=target,
            send_sem=halo_send.at[i],
            recv_sem=halo_recv.at[i],
            device_id=(after, tp),
            device_id_type=MESH,
        )
        for i, (source, target) in enumerate(
            (
                (ref.at[:, pl.ds(rows - WIN, WIN)], ext.at[:, pl.ds(0, WIN)])
                for ref, ext in (
                    (key_ref, key_ext),
                    (val_ref, val_ext),
                    (docs_ref, docs_ext),
                )
            )
        )
    ]
    for copy in halo:
        copy.start()
    near_sends(0)
    far_sends(0, inner | home)
    far_sends(1, home & jnp.logical_not(inner))
    near_sends(1)
    near_sends(2)
    own_row(0)
    own_row(1)
    settle = [
        pltpu.make_async_copy(own[w], slab(w, sp), local_sem.at[6 + w]) for w in range(3)
    ]
    tap_pairs = ((gate_taps_ref, taps_gate), (value_taps_ref, taps_value))
    for i, (source, target) in enumerate(tap_pairs):
        settle.append(pltpu.make_async_copy(source, target, local_sem.at[9 + i]))
    taps = [
        pltpu.make_async_remote_copy(
            src_ref=source,
            dst_ref=target,
            send_sem=taps_send.at[i],
            recv_sem=taps_recv.at[i],
            device_id=(sp, sibling),
            device_id_type=MESH,
        )
        for i, (source, target) in enumerate(tap_pairs)
    ]

    @pl.when(home)
    def _():
        for copy in settle + taps:
            copy.start()

    own_core(0)
    own_core(1)
    own_core(2)
    for copy in fetch:
        copy.wait()

    line = lax.broadcasted_iota(jnp.int32, (LANES, LANES), 0)
    lane = lax.broadcasted_iota(jnp.int32, (LANES, LANES), 1)
    for b in range(1, rows // LANES + 1):
        row_doc = docs_ext[0:1, b * LANES : (b + 1) * LANES].astype(F32)
        doc_cols[b * LANES : (b + 1) * LANES, :] = jnp.broadcast_to(row_doc, (LANES, LANES)).T

    zero = jnp.zeros((HD, 2 * WIN), BF16)

    def pair_copy(i, block):
        return pltpu.make_async_remote_copy(
            src_ref=parts.at[block],
            dst_ref=parts_in.at[i],
            send_sem=rows_send.at[i],
            recv_sem=rows_recv.at[i],
            device_id=(sp, sibling),
            device_id_type=MESH,
        )

    def facing_copy():
        return pltpu.make_async_remote_copy(
            src_ref=parts.at[facing],
            dst_ref=parts_in.at[2],
            send_sem=rows_send.at[2],
            recv_sem=rows_recv.at[2],
            device_id=(sp, facing),
            device_id_type=MESH,
        )

    def attend_block(j, carry):
        b = 2 * lax.rem(x + 1 + j, 2) + lax.rem(core + 1 + j // 2, 2)

        @pl.when(b == 0)
        def _():
            for copy in halo:
                copy.wait_recv()

        start = pl.multiple_of(b * WIN, WIN)
        k = key_ext[:, pl.ds(start, 2 * WIN)]
        v = val_ext[:, pl.ds(start, 2 * WIN)]
        keys = jnp.concatenate(
            [jnp.concatenate([k, zero], axis=1), jnp.concatenate([zero, k], axis=1)], axis=0
        )
        values = jnp.concatenate(
            [jnp.concatenate([v, zero], axis=1), jnp.concatenate([zero, v], axis=1)], axis=0
        )
        query_doc = doc_cols[pl.ds(start + WIN, WIN), :]
        prev_doc = docs_ext[0:1, pl.ds(start, WIN)].astype(F32)
        this_doc = docs_ext[0:1, pl.ds(start + WIN, WIN)].astype(F32)
        prev_ok = (query_doc == prev_doc) & (lane > line) & (sp * rows + b * WIN > 0)
        this_ok = (query_doc == this_doc) & (lane <= line)
        bias = jnp.concatenate(
            [jnp.where(prev_ok, 0.0, -1e30), jnp.where(this_ok, 0.0, -1e30)], axis=1
        ).astype(F32)
        for pair in range(query_ref.shape[1] // LANES):
            block = queries[pl.ds(start, WIN), pair * LANES : (pair + 1) * LANES]
            both = jnp.dot(block, keys, preferred_element_type=F32)
            probs = []
            for side in (0, 1):
                scores = both[:, side * 2 * WIN : (side + 1) * 2 * WIN] * HD ** (-0.5) + bias
                sink = sink_ref[2 * pair + side]
                top = jnp.maximum(jnp.max(scores, axis=1, keepdims=True), sink)
                weights = jnp.exp(scores - top)
                total = jnp.sum(weights, axis=1, keepdims=True) + jnp.exp(sink - top)
                probs.append((weights / total).astype(BF16))
            heads[:, pair * LANES : (pair + 1) * LANES] = lax.dot_general(
                jnp.concatenate(probs, axis=1),
                values,
                (((1,), (1,)), ((), ())),
                preferred_element_type=F32,
            ).astype(BF16)
        for c in range(width // 512):
            parts[b, :, c * 512 : (c + 1) * 512] = jnp.dot(
                heads[...], proj[:, c * 512 : (c + 1) * 512], preferred_element_type=F32
            ).astype(BF16)

        @pl.when(j == 0)
        def _():
            pair_copy(0, 2 * (1 - x) + 1 - core).start()

        @pl.when(j == 1)
        def _():
            pair_copy(1, sibling).start()

        @pl.when(j == 2)
        def _():
            pair_copy(0, facing).wait_recv()
            parts[facing] = (parts[facing].astype(F32) + parts_in[0].astype(F32)).astype(BF16)
            facing_copy().start()

        return carry

    lax.fori_loop(0, n_tp, attend_block, 0)

    serve(EARLY)
    own_row(2)
    pair_copy(1, tp).wait_recv()
    facing_copy().wait_recv()
    first = mix_scale * rest[...].astype(F32) + parts[tp].astype(F32)
    first = first + parts_in[1].astype(F32) + parts_in[2].astype(F32)
    mean = jnp.mean(first, axis=1, keepdims=True)
    first = first - mean
    var = jnp.mean(first * first, axis=1, keepdims=True)
    norm_own[...] = (first * lax.rsqrt(var + norm_eps) * mix_ref[...]).astype(BF16)

    def workers(block):
        parity = lax.rem(block // 2, 2)
        return [
            (block - 2 * parity + 2 * a, 2 * b + parity)
            for a in (0, 1)
            for b in range(n_tp // 2)
        ]

    def place_of(source):
        return pl.ds(pl.multiple_of(PAD + source * row_share, PAD), row_share)

    def norm_copy(i, device, source):
        return pltpu.make_async_remote_copy(
            src_ref=norm_own,
            dst_ref=normed.at[place_of(source)],
            send_sem=norm_send.at[i],
            recv_sem=norm_recv.at[source],
            device_id=device,
            device_id_type=MESH,
        )

    def takes(i, device):
        return jnp.where(device[0] == sp, device[1] != tp, x == i % 2)

    def norm_pass(i):
        return pltpu.make_async_remote_copy(
            src_ref=normed.at[place_of(2 * x + i)],
            dst_ref=normed.at[place_of(2 * x + i)],
            send_sem=pass_send.at[i],
            recv_sem=norm_recv.at[2 * x + i],
            device_id=(sp, facing),
            device_id_type=MESH,
        )

    def cols_copy(i, peer, source):
        rows_at = pl.ds(pl.multiple_of(source * row_share, row_share), row_share)
        return pltpu.make_async_remote_copy(
            src_ref=norm_own.at[:, pl.ds(pl.multiple_of(peer * share, share), share)],
            dst_ref=norm_cols.at[rows_at],
            send_sem=cols_send.at[i],
            recv_sem=cols_recv.at[source],
            device_id=(sp, peer),
            device_id_type=MESH,
        )

    def tail_copy(i, device):
        return pltpu.make_async_remote_copy(
            src_ref=norm_own.at[pl.ds(row_share - PAD // 2, PAD // 2)],
            dst_ref=normed.at[pl.ds(PAD // 2, PAD // 2)],
            send_sem=tail_send.at[i],
            recv_sem=tail_recv,
            device_id=device,
            device_id_type=MESH,
        )

    own_workers = workers(sp)
    next_workers = workers(after)

    @pl.when((tp == n_tp - 1) & (sp < n - 1))
    def _():
        for i, device in enumerate(next_workers):
            tail_copy(i, device).start()

    for i, device in enumerate(own_workers):
        @pl.when(takes(i, device))
        def _():
            norm_copy(i, device, tp).start()

    far_sends(2, home & jnp.logical_not(inner))
    for i, peer in enumerate(peers):
        cols_copy(i, peer, tp).start()

    docs_copy = pltpu.make_async_remote_copy(
        src_ref=docs_ext,
        dst_ref=docs_other,
        send_sem=halo_send.at[3],
        recv_sem=halo_recv.at[3],
        device_id=(partner, tp),
        device_id_type=MESH,
    )
    docs_copy.start()

    @pl.when(home)
    def _():
        normed[place_of(tp), :] = norm_own[...]

    norm_cols[pl.ds(pl.multiple_of(tp * row_share, row_share), row_share), :] = norm_own[
        :, pl.ds(pl.multiple_of(tp * share, share), share)
    ]

    serve(MIDDLE)
    docs_copy.wait_recv()
    place = lax.broadcasted_iota(jnp.int32, (LANES, LANES), 0)
    for b in range(rows // LANES):
        now = slice(WIN + b * LANES, WIN + (b + 1) * LANES)
        before = slice(b * LANES, (b + 1) * LANES)
        doc_now = jnp.where(home, docs_ext[0:1, now], docs_other[0:1, now]).astype(F32)
        doc_before = jnp.where(home, docs_ext[0:1, before], docs_other[0:1, before]).astype(F32)
        tall = jnp.broadcast_to(doc_now, (LANES, LANES)).T
        ahead = jnp.broadcast_to(doc_before, (LANES, LANES)).T
        mask_cols[0, PAD + b * LANES : PAD + (b + 1) * LANES, :] = tall
        if b == 0:
            mask_cols[0, 0:PAD, :] = ahead[LANES - PAD :]
    for b in range(rows // LANES):
        at = PAD + b * LANES
        doc = mask_cols[0, at : at + LANES, :]
        for lag in range(1, TAPS):
            same = (mask_cols[0, at - lag : at - lag + LANES, :] == doc) & (
                place + (work * rows + b * LANES) >= lag
            )
            mask_cols[lag, at : at + LANES, :] = jnp.where(same, 1.0, 0.0).astype(F32)

    for source in range(n_tp):
        @pl.when(jnp.where(home, tp != source, x != source // 2))
        def _():
            norm_copy(0, (sp, sibling), source).wait_recv()

    @pl.when(work > 0)
    def _():
        tail_copy(0, (sp, sibling)).wait_recv()

    @pl.when(work == 0)
    def _():
        normed[0:PAD, :] = jnp.zeros((PAD, width), BF16)


    @pl.when(home)
    def _():
        for copy in settle:
            copy.wait()

    @pl.when(jnp.logical_not(home))
    def _():
        for copy in taps:
            copy.wait_recv()

    for w in (0, 1):
        for k in range(planes):
            for flip in (0, 1):
                await_slab(w, k, flip)

    def convolved(source, taps_ref, at):
        total = taps_ref[0:1, pl.ds(at, LANES)] * source[PAD : PAD + rows, :]
        for lag in range(1, TAPS):
            tap = taps_ref[lag : lag + 1, pl.ds(at, LANES)]
            shifted = source[PAD - lag : PAD - lag + rows, :]
            total = total + tap * (shifted * mask_cols[lag, PAD : PAD + rows, :])
        return total

    def project(c, pair):
        at = pl.multiple_of(c * LANES, LANES)
        weights = jnp.concatenate(
            [gate_all[:, pl.ds(at, LANES)], value_all[:, pl.ds(at, LANES)]], axis=1
        )
        both = jnp.dot(normed[...], weights, preferred_element_type=F32)
        both = both.astype(BF16).astype(F32)
        pair[0][...] = both[:, :LANES]
        pair[1][...] = both[:, LANES:]

    def activate(c, pair):
        at = pl.multiple_of(c * LANES, LANES)
        gate = convolved(pair[0], taps_gate, at)
        value = convolved(pair[1], taps_value, at)
        inside = math.sqrt(2.0 / math.pi) * (gate + 0.044715 * (gate * gate * gate))
        hidden[:, pl.ds(at, LANES)] = (0.5 * gate * (1.0 + jnp.tanh(inside)) * value).astype(BF16)

    even, odd = (up_gate.at[0], up_value.at[0]), (up_gate.at[1], up_value.at[1])
    steps = ff // LANES
    project(0, even)

    def up_block(d, carry):
        c = 2 * d
        activate(c, even)
        project(c + 1, odd)
        activate(c + 1, odd)
        project(c + 2, even)
        for at_step, events in UP_SERVE:
            @pl.when(d == at_step)
            def _():
                serve(events)

        return carry

    lax.fori_loop(0, (steps - 1) // 2, up_block, 0)
    activate(steps - 1, even)

    def term_copy(index, target, where, sem, device):
        return pltpu.make_async_remote_copy(
            src_ref=terms.at[index],
            dst_ref=target.at[where],
            send_sem=term_send.at[index],
            recv_sem=sem.at[where],
            device_id=device,
            device_id_type=MESH,
        )

    def to_owner(index, source, device):
        return term_copy(index, terms_in, per * source + lax.rem(index, per), term_recv, device)

    def to_mate(index, over_x):
        device = (sp, facing) if over_x else (work, tp)
        return term_copy(index, from_mate, lax.rem(index, 2 * per), mate_recv, device)

    def slab_index(k, flip):
        return 2 * zone(k) + (1 - y if flip else y)

    def down_block(k, flip):
        index = slab_index(k, flip)
        owner = index // per
        crossing = owner // 2 != x
        serve(DOWN_SERVE.get((k, flip), ()))
        await_slab(2, k, flip)
        terms[index] = jnp.dot(
            hidden[...], down_all[index], preferred_element_type=F32
        ).astype(BF16)

        @pl.when(home & (owner == tp))
        def _():
            terms_in[lax.rem(index, per)] = terms[index]

        @pl.when(home & (owner == sibling))
        def _():
            to_owner(index, 0, (sp, sibling)).start()

        if (k, flip) in X_FIRST:
            @pl.when(home & crossing)
            def _():
                to_owner(index, 2, (sp, owner)).start()
        else:
            @pl.when(jnp.logical_not(home | crossing))
            def _():
                to_owner(index, 1, (work, owner)).start()

        @pl.when(jnp.logical_not(home) & crossing)
        def _():
            to_mate(index, (k, flip) in X_FIRST).start()

    def cross_block(k, flip):
        index = slab_index(k, flip)
        owner = index // per

        crossing = owner // 2 != x

        over_x = (k, flip) in X_FIRST

        @pl.when(jnp.logical_not(home | crossing) if over_x else home & crossing)
        def _():
            to_mate(index, over_x).wait_recv()
            terms[index] = (
                terms[index].astype(F32) + from_mate[lax.rem(index, 2 * per)].astype(F32)
            ).astype(BF16)
            if over_x:
                to_owner(index, 1, (work, owner)).start()
            else:
                to_owner(index, 2, (sp, owner)).start()

    for step, k, flip in DOWN_ORDER:
        (down_block if step == "down" else cross_block)(k, flip)

    for source in range(3):
        @pl.when(jnp.logical_not(home) if source == 0 else tp >= 0)
        def _():
            for j in range(per):
                term_copy(
                    0, terms_in, per * source + j, term_recv, (sp, sibling)
                ).wait_recv()

    for i, peer in enumerate(peers):
        cols_copy(i, peer, peer).wait_recv()

    sums = jnp.zeros((rows, 1), F32)
    squares = jnp.zeros((rows, 1), F32)
    for j in range(per):
        total = mix_scale * norm_cols[:, j * cols : (j + 1) * cols].astype(F32)
        for source in range(3):
            total = total + terms_in[per * source + j].astype(F32)
        second[:, j * cols : (j + 1) * cols] = total
        sums = sums + jnp.sum(total, axis=1, keepdims=True)
        squares = squares + jnp.sum(total * total, axis=1, keepdims=True)
    which = lax.broadcasted_iota(jnp.int32, (rows, LANES), 1)
    packed = jnp.where(which == 0, sums, jnp.where(which == 1, squares, 0.0))
    stats[tp] = packed.T[0:8]

    def stat_copy(peer, source):
        return pltpu.make_async_remote_copy(
            src_ref=stats.at[source],
            dst_ref=stats.at[source],
            send_sem=stat_send.at[peer],
            recv_sem=stat_recv.at[source],
            device_id=(sp, peer),
            device_id_type=MESH,
        )

    for peer in peers:
        stat_copy(peer, tp).start()

    for w in range(3):
        for i in range(2):
            @pl.when((core + 2 * i != z) & ((half == i) | inner | home))
            def _():
                for q in range(CHUNKS):
                    to_plane(w, i, q).wait_send()

        @pl.when(inner)
        def _():
            for i in range(CHUNKS // 2):
                onward(w, i).wait_send()

    for k in range(planes):
        at = zone(k)
        for w in range(3):
            for i in range(CHUNKS // 2):
                q = 2 * i + role
                if k > 0:
                    index = 2 * at + y
                    to_row(w, at, q, slot(w, index, q), tp).wait_send()
                    to_core(w, index, q, slot(w, index, q)).wait_send()
                index = 2 * at + 1 - y
                to_core(w, index, q, slot(w, index, q)).wait_send()

    @pl.when(home)
    def _():
        for w in range(3):
            for q in range(CHUNKS):
                to_row(w, z, q, piece(w, q), tp if q % 2 == 0 else sibling).wait_send()
                to_core(w, sp, q, piece(w, q)).wait_send()
        for copy in taps:
            copy.wait_send()

    for copy in halo:
        copy.wait_send()
    docs_copy.wait_send()
    for i, device in enumerate(own_workers):
        @pl.when(takes(i, device))
        def _():
            norm_copy(i, device, tp).wait_send()

    @pl.when(jnp.logical_not(home))
    def _():
        for i in PAIR:
            norm_pass(i).wait_send()

    @pl.when((tp == n_tp - 1) & (sp < n - 1))
    def _():
        for i, device in enumerate(next_workers):
            tail_copy(i, device).wait_send()

    pair_copy(0, 2 * (1 - x) + 1 - core).wait_send()
    pair_copy(1, sibling).wait_send()
    facing_copy().wait_send()
    for i, peer in enumerate(peers):
        cols_copy(i, peer, tp).wait_send()
    for index in range(n):
        @pl.when(jnp.logical_not(home & (tp == index // per)))
        def _():
            to_mate(index, 0).wait_send()

    for peer in peers:
        stat_copy(peer, peer).wait_recv()
    total = stats[0]
    for source in range(1, n_tp):
        total = total + stats[source]
    spread = jnp.concatenate([total] * (LANES // 8), axis=0).T
    mean = spread[:, 0:1] / width
    var = spread[:, 1:2] / width - mean * mean
    out_ref[...] = (
        (second[...] - mean) * lax.rsqrt(var + norm_eps) * final_ref[...]
    ).astype(BF16)
    for peer in peers:
        stat_copy(peer, tp).wait_send()


def fused(
    query_rows,
    key_rows,
    value_rows,
    doc_ids,
    sink_logit,
    residual,
    out_proj,
    mix_gain,
    gate_proj,
    value_proj,
    gate_taps,
    value_taps,
    down_proj,
    final_gain,
):
    n = lax.axis_size("sp")
    n_tp = lax.axis_size("tp")
    rows, head_cols = query_rows.shape
    width = residual.shape[1]
    depth, ff = gate_proj.shape
    cols = down_proj.shape[1]
    per = width // n_tp // cols
    planes = n // 2
    share = rows // n_tp
    anywhere = pl.BlockSpec(memory_space=pl.ANY)
    vmem = pl.BlockSpec(memory_space=pltpu.VMEM)
    smem = pl.BlockSpec(memory_space=pltpu.SMEM)
    dma = pltpu.SemaphoreType.DMA
    return pl.pallas_call(
        functools.partial(layer_kernel, n, n_tp),
        out_shape=jax.ShapeDtypeStruct((rows, width // n_tp), BF16),
        in_specs=[
            anywhere, anywhere, anywhere, smem, anywhere, anywhere, anywhere, vmem,
            anywhere, anywhere, anywhere, anywhere, anywhere, vmem,
        ],
        out_specs=vmem,
        scratch_shapes=[
            pltpu.VMEM((n * depth, ff), BF16),
            pltpu.VMEM((n * depth, ff), BF16),
            pltpu.VMEM((n, ff, cols), BF16),
            pltpu.VMEM((HD, WIN + rows), BF16),
            pltpu.VMEM((HD, WIN + rows), BF16),
            pltpu.VMEM((1, WIN + rows), jnp.int32),
            pltpu.VMEM((1, WIN + rows), jnp.int32),
            pltpu.VMEM((WIN + rows, LANES), F32),
            pltpu.VMEM((TAPS, PAD + rows, LANES), F32),
            pltpu.VMEM(gate_taps.shape, F32),
            pltpu.VMEM(value_taps.shape, F32),
            pltpu.VMEM((rows, head_cols), BF16),
            pltpu.VMEM((head_cols, width), BF16),
            pltpu.VMEM((share, width), BF16),
            pltpu.VMEM((share, head_cols), BF16),
            pltpu.VMEM((n_tp, share, width), BF16),
            pltpu.VMEM((3, share, width), BF16),
            pltpu.VMEM((share, width), BF16),
            pltpu.VMEM((rows, width // n_tp), BF16),
            pltpu.VMEM((PAD + rows, width), BF16),
            pltpu.VMEM((2, PAD + rows, LANES), F32),
            pltpu.VMEM((2, PAD + rows, LANES), F32),
            pltpu.VMEM((rows, ff), BF16),
            pltpu.VMEM((n, rows, cols), BF16),
            pltpu.VMEM((3 * per, rows, cols), BF16),
            pltpu.VMEM((2 * per, rows, cols), BF16),
            pltpu.VMEM((rows, width // n_tp), F32),
            pltpu.VMEM((n_tp, 8, rows), F32),
            dma((3, 2, CHUNKS)),
            dma((3, CHUNKS // 2)),
            dma((3, planes, CHUNKS)),
            dma((3, n, CHUNKS)),
            dma((3, n, CHUNKS)),
            dma((3, n, CHUNKS)),
            dma((11,)),
            dma((2,)),
            dma((2,)),
            dma((4,)),
            dma((4,)),
            dma((3,)),
            dma((3,)),
            dma((n_tp,)),
            dma((n_tp,)),
            dma((2,)),
            dma((n_tp,)),
            dma((n_tp,)),
            dma((n_tp,)),
            dma(()),
            dma((n,)),
            dma((3 * per,)),
            dma((2 * per,)),
            dma((n_tp,)),
            dma((n_tp,)),
        ],
        compiler_params=pltpu.CompilerParams(
            collective_id=0, has_side_effects=True, vmem_limit_bytes=60 * 1024 * 1024
        ),
        name="layer",
    )(
        key_rows.T,
        value_rows.T,
        doc_ids[None, :],
        sink_logit,
        query_rows,
        out_proj,
        residual,
        mix_gain[None, :],
        gate_proj,
        value_proj,
        gate_taps,
        value_taps,
        down_proj,
        final_gain[None, :],
    )


def on_any(*args):
    query_rows, key_rows, gate_proj, down_proj = args[0], args[1], args[8], args[12]
    n, n_tp = lax.axis_size("sp"), lax.axis_size("tp")
    share = args[5].shape[1] // n_tp
    depth, ff = gate_proj.shape
    cols = down_proj.shape[1]
    fits = (
        n == 8
        and n_tp == 4
        and ff >= 10 * LANES
        and query_rows.shape[0] == n_tp * WIN
        and key_rows.shape[1] == HD
        and query_rows.shape[1] % LANES == 0
        and depth % (16 * CHUNKS) == 0
        and ff % (2 * LANES) == LANES
        and ff % (16 * CHUNKS) == 0
        and cols % LANES == 0
        and share % cols == 0
    )
    return fused(*args) if fits else on_device(*args)


def solution(mesh):
    placed = (
        P("sp", "tp"),
        P("sp", "tp"),
        P("sp", "tp"),
        P("sp"),
        P("tp"),
        P("sp", None),
        P("tp", None),
        P(),
        P("sp", "tp"),
        P("sp", "tp"),
        P(None, "tp"),
        P(None, "tp"),
        P("tp", "sp"),
        P("tp"),
    )
    return jax.shard_map(
        on_any, mesh=mesh, in_specs=placed, out_specs=P("sp", "tp"), check_vma=False
    )
```
